256 devices in a mesh: ep: 64 (over z, x, core), tp: 4 (over y).
Axes of the slice: x: 4, y: 4, z: 8, core: 2. Of those that a mesh axis runs over, the one named last changes fastest.
Arguments:
- x_attend: bfloat16 [32768, 2048], P('ep'), may hold values from -6 to 6
- attend_gain: float32 [2048], replicated, may hold values from 0.1 to 1.9
- w_query: bfloat16 [2048, 1024], P(None, 'tp'), may hold values from -0.125 to 0.125
- w_key: bfloat16 [2048, 512], P(None, 'tp'), may hold values from -0.125 to 0.125
- w_value: bfloat16 [2048, 512], P(None, 'tp'), may hold values from -0.125 to 0.125
- query_gain: float32 [64], replicated, may hold values from 0.1 to 1.9
- key_gain: float32 [64], replicated, may hold values from 0.1 to 1.9
- sink_logit: float32 [16], P('tp'), may hold values from 4 to 8
- w_output: bfloat16 [1024, 2048], P('tp'), may hold values from -1.5 to 1.5
- x_experts: bfloat16 [24576, 2048], P('ep'), may hold values from -6 to 6
- expert_gain: float32 [2048], replicated, may hold values from 0.1 to 1.9
- routes: int32 [24576, 2], P('ep'), may hold values from 0 to 63, all different within a row; in each aligned block of 384 rows (0 to 383, 384 to 767, ...) at most 18 rows name the same one
- group_prob: float32 [24576], P('ep'), may hold values from 0.3 to 1
- expert_prob: float32 [24576, 2], P('ep'), may hold values from 0.05 to 1
- w_gate: bfloat16 [64, 2048, 1024], P('ep', None, 'tp'), may hold values from -0.125 to 0.125
- w_up: bfloat16 [64, 2048, 1024], P('ep', None, 'tp'), may hold values from -0.125 to 0.125
- w_down: bfloat16 [64, 1024, 2048], P('ep', 'tp'), may hold values from -0.1875 to 0.1875
Outputs:
- attend_out: bfloat16 [32768, 2048], P(('ep', 'tp'))
- expert_out: bfloat16 [24576, 2048], P('ep', 'tp')
The draws below stay inside these ranges and needn't reach their ends.
Inputs may be any that keep to these rules, and one draw needn't show every extreme that they name: `routes`: each row names 2 different experts. Among the rows of one device no expert is named more than 18 times, and in every draw some expert is named exactly 18 times by one device's rows.
All inputs are finite; a program needn't handle non-finite values.
Results may differ from the reference program's by a relative error of at most 0.012.
Values may be sent and summed in bfloat16 or wider, within the bound.
A program may use at most 64 MiB of HBM per device.

```python
import math
import jax
import jax.numpy as jnp
import numpy as np
from jax import lax

D = 2048
HEADS = 16
KV_HEADS = 8
HEAD_DIM = 64
FF = 1024
TOPK = 2
WINDOW = 128
GRID_W = 64
TOK_A = 512
TOK_M = 384
EXPERTS = 64
CAP = 18
TOKENS_A = 32768
TOKENS_M = 24576
N_EP = 64
N_TP = 4


def levels(rng, shape, pieces, smallest, high):
    factor_of = 1.0
    for dim, blocks in pieces:
        heights = jax.random.uniform(jax.random.fold_in(jax.random.fold_in(rng, 6), dim), (blocks,), jnp.float32, smallest / len(pieces), high / len(pieces))
        factor_of = factor_of * jnp.repeat(jnp.exp(heights), shape[dim] // blocks).reshape((-1,) + (1,) * (len(shape) - 1 - dim))
    return factor_of


def assign_block(rng, own, number, rows, amount, top, reach, slope):
    ranking = jax.random.permutation(rng, amount)
    heavy_load, ordinary = shares(amount, rows * top, reach, slope, True), shares(amount, rows * top, reach, slope, False)
    places = jnp.arange(amount)

    def named(tallies, offset_by):
        used = int((tallies > 0).sum())
        fixed = max(1, used // 4)
        moved = fixed + (places - fixed + offset_by * (used - fixed)) % max(1, amount - fixed)
        return jnp.zeros((amount,), jnp.int32).at[ranking[jnp.where(places < fixed, places, moved)]].set(jnp.asarray(tallies, jnp.int32))

    tallies = jnp.where(number % 4 == 0, named(heavy_load, number // 4), named(ordinary, number - number // 4 - 1))
    mixed = jax.random.permutation(jax.random.fold_in(own, 3), amount)
    giver, sink = mixed[0:amount // 2 * 2:2], mixed[1:amount // 2 * 2:2]
    slack = jnp.minimum(tallies[giver] - 1, reach - tallies[sink]) // 2
    slack = jnp.where((giver == ranking[0]) | (sink == ranking[0]) | (tallies[sink] == 0), 0, jnp.maximum(slack, 0))
    moved = jax.random.randint(jax.random.fold_in(own, 4), (amount // 2,), 0, 1 << 20) % (slack + 1)
    tallies = tallies.at[giver].add(-moved).at[sink].add(moved)
    labels = jnp.searchsorted(jnp.cumsum(tallies), jnp.arange(rows * top), side="right").astype(jnp.int32)
    listing = labels.reshape(top, rows).T
    listing = listing[jax.random.permutation(jax.random.fold_in(own, 1), rows)]
    offset_by = jax.random.randint(jax.random.fold_in(own, 2), (rows, 1), 0, top)
    return jnp.take_along_axis(listing, (jnp.arange(top)[None, :] + offset_by) % top, axis=1)


def shares(amount, total, reach, skew, full):
    loads = [(1 << 20) // math.isqrt(grade ** skew) + 1 for grade in range(1, amount + 1)]
    largest = reach if full else min(reach, max(-(-total // amount), total * loads[0] // sum(loads)))
    least = 1 if total - largest >= amount - 1 else 0
    holding, surplus = [largest] + [least] * (amount - 1), total - largest - least * (amount - 1)
    while surplus > 0:
        free = [i for i in range(1, amount) if holding[i] < largest] or [i for i in range(1, amount) if holding[i] < reach]
        whole, remaining = sum([loads[i] for i in free]), surplus
        for i in free:
            extra = min(reach - holding[i], max(1, remaining * loads[i] // whole), surplus)
            holding[i] = holding[i] + extra
            surplus = surplus - extra
    return np.array(holding)


def gaussian(key, dims, width, bound, cuts=(), kind=jnp.bfloat16):
    level = levels(key, dims, cuts, -0.22, 0.18) if cuts else 1.0
    values = jax.random.normal(key, dims, jnp.float32) * width * level
    return jnp.minimum(jnp.maximum(values, -bound), bound).astype(kind)


def setup_inputs(seed: int = 0) -> dict:
    arg_keys = jax.random.split(jax.random.key(seed), 18)
    x_attend = gaussian(arg_keys[0], (TOKENS_A, D), 1.0, 6.0, ((0, 64),))
    attend_gain = jnp.clip(1.0 + 0.18 * jax.random.normal(arg_keys[1], (D,), jnp.float32), 0.1, 1.9)
    w_query = gaussian(arg_keys[2], (D, HEADS * HEAD_DIM), D ** -0.5, 0.125, ((1, 4),))
    w_key = gaussian(arg_keys[3], (D, KV_HEADS * HEAD_DIM), D ** -0.5, 0.125, ((1, 4),))
    w_value = gaussian(arg_keys[4], (D, KV_HEADS * HEAD_DIM), D ** -0.5, 0.125, ((1, 4),))
    query_gain = jnp.clip(1.0 + 0.18 * jax.random.normal(arg_keys[5], (HEAD_DIM,), jnp.float32), 0.1, 1.9)
    key_gain = jnp.clip(1.0 + 0.18 * jax.random.normal(arg_keys[6], (HEAD_DIM,), jnp.float32), 0.1, 1.9)
    sink_logit = jnp.clip(4.0 + 4.0 * jax.random.uniform(arg_keys[7], (HEADS,), jnp.float32) ** levels(arg_keys[7], (HEADS,), ((0, 4),), -0.2, 0.2), 4.0, 8.0)
    w_output = gaussian(arg_keys[8], (HEADS * HEAD_DIM, D), (HEAD_DIM // 4) ** -0.5, 1.5, ((0, 4),))
    x_experts = gaussian(arg_keys[9], (TOKENS_M, D), 1.0, 6.0, ((0, 64),))
    expert_gain = jnp.clip(1.0 + 0.18 * jax.random.normal(arg_keys[10], (D,), jnp.float32), 0.1, 1.9)
    routes_keys = jax.random.split(jax.random.fold_in(arg_keys[11], 1), TOKENS_M // TOK_M)
    routes_turns = jax.random.permutation(jax.random.fold_in(arg_keys[11], 3), TOKENS_M // TOK_M)
    routes = jax.vmap(lambda own, number: assign_block(jax.random.fold_in(arg_keys[11], 2), own, number, TOK_M, EXPERTS, TOPK, CAP, 2))(routes_keys, routes_turns).reshape((TOKENS_M, TOPK))
    group_prob = jnp.clip(0.3 + 0.7 * jax.random.uniform(arg_keys[12], (TOKENS_M,), jnp.float32) ** levels(arg_keys[12], (TOKENS_M,), ((0, 64),), -0.2, 0.2), 0.3, 1.0)
    expert_prob = jnp.clip(0.05 + 0.95 * jax.random.uniform(arg_keys[13], (TOKENS_M, TOPK), jnp.float32) ** levels(arg_keys[13], (TOKENS_M, TOPK), ((0, 64),), -0.2, 0.2), 0.05, 1.0)
    w_gate = gaussian(arg_keys[14], (EXPERTS, D, FF), D ** -0.5, 0.125, ((0, 64), (2, 4)))
    w_up = gaussian(arg_keys[15], (EXPERTS, D, FF), D ** -0.5, 0.125, ((0, 64), (2, 4)))
    w_down = gaussian(arg_keys[16], (EXPERTS, FF, D), FF ** -0.5, 0.1875, ((0, 64), (1, 4)))
    return dict(x_attend=x_attend, attend_gain=attend_gain, w_query=w_query, w_key=w_key, w_value=w_value, query_gain=query_gain, key_gain=key_gain, sink_logit=sink_logit, w_output=w_output, x_experts=x_experts, expert_gain=expert_gain, routes=routes, group_prob=group_prob, expert_prob=expert_prob, w_gate=w_gate, w_up=w_up, w_down=w_down)


epsilon = 1e-06
rope_base = 10000.0

def rms_scale(inputs, gain):
    values_f = inputs.astype(jnp.float32)
    scaled = values_f * lax.rsqrt(lax.optimization_barrier(jnp.mean(values_f * values_f, axis=-1, keepdims=True)) + epsilon)
    return (scaled * gain).astype(jnp.bfloat16)

def rope_tables(positions):
    grid_rows = (positions // GRID_W).astype(jnp.float32)
    grid_cols = (positions % GRID_W).astype(jnp.float32)
    half_dim = HEAD_DIM // 2
    inverse = rope_base ** (-jnp.arange(0, half_dim, 2, dtype=jnp.float32) / half_dim)
    angles = jnp.concatenate([grid_rows[:, None] * inverse, grid_cols[:, None] * inverse], axis=-1)
    return (jnp.cos(angles), jnp.sin(angles))

def head_norm_rope(projected, gain, cosine, sine_tab):
    scaled = projected * lax.rsqrt(lax.optimization_barrier(jnp.mean(projected * projected, axis=-1, keepdims=True)) + epsilon) * gain
    first_half, second_half = jnp.split(scaled, 2, axis=-1)
    cos_b = cosine[:, None, :]
    sin_b = sine_tab[:, None, :]
    turned = jnp.concatenate([first_half * cos_b - second_half * sin_b, second_half * cos_b + first_half * sin_b], axis=-1)
    return turned.astype(jnp.bfloat16)

def slot_plan(route_block):
    flat_ids = route_block.reshape(-1).astype(jnp.int32)
    onehot = (flat_ids[:, None] == jnp.arange(EXPERTS, dtype=jnp.int32)[None, :]).astype(jnp.int32)
    rank_in = jnp.cumsum(onehot, axis=0) - onehot
    slot_pos = lax.optimization_barrier(jnp.sum(rank_in * onehot, axis=1))
    dest_slot = (flat_ids * CAP + slot_pos).astype(jnp.int32)
    owner_tok = (jnp.arange(TOK_M * TOPK, dtype=jnp.int32) // TOPK).astype(jnp.int32)
    slot_tok = jnp.full((EXPERTS * CAP,), TOK_M, jnp.int32).at[dest_slot].set(owner_tok)
    return (dest_slot, slot_tok)

def reference(x_attend, attend_gain, w_query, w_key, w_value, query_gain, key_gain, sink_logit, w_output, x_experts, expert_gain, routes, group_prob, expert_prob, w_gate, w_up, w_down):
    normed = rms_scale(x_attend, attend_gain)
    positions = jnp.arange(TOKENS_A, dtype=jnp.int32)
    cosine, sine_tab = rope_tables(positions)
    queries = head_norm_rope(jnp.dot(normed, w_query, preferred_element_type=jnp.float32).reshape(TOKENS_A, HEADS, HEAD_DIM), query_gain, cosine, sine_tab)
    key_rows = head_norm_rope(jnp.dot(normed, w_key, preferred_element_type=jnp.float32).reshape(TOKENS_A, KV_HEADS, HEAD_DIM), key_gain, cosine, sine_tab)
    values = jnp.dot(normed, w_value, preferred_element_type=jnp.float32).astype(jnp.bfloat16).reshape(TOKENS_A, KV_HEADS, HEAD_DIM)
    key_pad = jnp.pad(key_rows, ((WINDOW, WINDOW), (0, 0), (0, 0)))
    value_pad = jnp.pad(values, ((WINDOW, WINDOW), (0, 0), (0, 0)))
    group = HEADS // KV_HEADS
    sink_col = sink_logit.reshape(KV_HEADS, group)[:, :, None]

    def one_block(blk_idx):
        row_zero = (blk_idx * TOK_A).astype(jnp.int32)
        query_blk = lax.dynamic_slice_in_dim(queries, row_zero, TOK_A, 0).reshape(TOK_A, KV_HEADS, group, HEAD_DIM).astype(jnp.float32)
        key_blk = lax.dynamic_slice_in_dim(key_pad, row_zero, TOK_A + 2 * WINDOW, 0).astype(jnp.float32)
        value_blk = lax.dynamic_slice_in_dim(value_pad, row_zero, TOK_A + 2 * WINDOW, 0).astype(jnp.float32)
        scores = jnp.einsum('qhgd,khd->hgqk', query_blk, key_blk) * HEAD_DIM ** (-0.5)
        query_pos = row_zero + jnp.arange(TOK_A, dtype=jnp.int32)
        key_pos = row_zero - WINDOW + jnp.arange(TOK_A + 2 * WINDOW, dtype=jnp.int32)
        in_window = (jnp.abs(query_pos[:, None] - key_pos[None, :]) <= WINDOW) & (key_pos[None, :] >= 0) & (key_pos[None, :] < TOKENS_A)
        scores = jnp.where(in_window[None, None], scores, -1e+30)
        peak = jnp.maximum(lax.optimization_barrier(jnp.max(scores, axis=-1)), sink_col)[..., None]
        weights = jnp.exp(scores - peak)
        denominator = lax.optimization_barrier(jnp.sum(weights, axis=-1, keepdims=True)) + jnp.exp(sink_col[..., None] - peak)
        probs = (weights / denominator).astype(jnp.bfloat16)
        attended_blk = jnp.einsum('hgqk,khd->qhgd', probs.astype(jnp.float32), value_blk)
        return attended_blk.astype(jnp.bfloat16).reshape(TOK_A, HEADS * HEAD_DIM)
    attended = lax.map(one_block, jnp.arange(N_EP, dtype=jnp.int32)).reshape(TOKENS_A, HEADS * HEAD_DIM)
    head_cols = HEADS * HEAD_DIM // N_TP
    total = jnp.zeros((TOKENS_A, D), jnp.float32)
    for part_idx in range(N_TP):
        partial_value = jnp.dot(attended[:, part_idx * head_cols:(part_idx + 1) * head_cols], w_output[part_idx * head_cols:(part_idx + 1) * head_cols], preferred_element_type=jnp.float32)
        partial_value = lax.optimization_barrier(partial_value.astype(jnp.bfloat16))
        total = total + partial_value.astype(jnp.float32)
    attend_out = total.astype(jnp.bfloat16)
    moe_normed = rms_scale(x_experts, expert_gain).reshape(N_EP, TOK_M, D)
    route_blocks = routes.reshape(N_EP, TOK_M, TOPK)
    dest_slot, slot_tok = jax.vmap(slot_plan)(route_blocks)
    padded_rows = jnp.concatenate([moe_normed, jnp.zeros((N_EP, 1, D), jnp.bfloat16)], axis=1)
    outgoing = jax.vmap(lambda rows_all, index_all: rows_all[index_all])(padded_rows, slot_tok)
    inbound = outgoing.reshape(N_EP, EXPERTS, CAP, D).transpose(1, 0, 2, 3)
    unit_cols = FF // N_TP

    def one_expert(operands):
        rows_in, gate_mat, up_mat, down_mat = operands
        flat_rows = rows_in.reshape(N_EP * CAP, D)
        gate_act = jnp.dot(flat_rows, gate_mat, preferred_element_type=jnp.float32)
        up_act = jnp.dot(flat_rows, up_mat, preferred_element_type=jnp.float32)
        hidden = (jax.nn.silu(gate_act) * up_act).astype(jnp.bfloat16)
        summed = jnp.zeros((N_EP * CAP, D), jnp.float32)
        for part_idx in range(N_TP):
            partial_value = jnp.dot(hidden[:, part_idx * unit_cols:(part_idx + 1) * unit_cols], down_mat[part_idx * unit_cols:(part_idx + 1) * unit_cols], preferred_element_type=jnp.float32)
            partial_value = lax.optimization_barrier(partial_value.astype(jnp.bfloat16))
            summed = summed + partial_value.astype(jnp.float32)
        return summed.astype(jnp.bfloat16).reshape(N_EP, CAP, D)
    results = lax.map(one_expert, (inbound, w_gate, w_up, w_down))
    back_rows = results.transpose(1, 0, 2, 3).reshape(N_EP, EXPERTS * CAP, D)
    picked = jax.vmap(lambda rows_all, index_all: rows_all[index_all])(back_rows, dest_slot).astype(jnp.float32)
    route_weight = group_prob[:, None] * expert_prob / lax.optimization_barrier(jnp.sum(expert_prob, axis=1, keepdims=True))
    expert_out = lax.optimization_barrier(jnp.sum(picked.reshape(TOKENS_M, TOPK, D) * route_weight[:, :, None], axis=1)).astype(jnp.bfloat16)
    return (attend_out, expert_out)
```

```python
import functools

import jax
import jax.numpy as jnp
import numpy as np
from jax import lax
from jax.experimental import pallas as pl
from jax.experimental.pallas import tpu as pltpu
from jax.sharding import PartitionSpec as P

HEAD_DIM = 64
WINDOW = 128
GRID_W = 64
MAIN = 16
EXTRA = 2

epsilon = 1e-06
rope_base = 10000.0

BF = jnp.bfloat16
F32 = jnp.float32
MESH = pl.DeviceIdType.MESH


def dot(a, b):
    return jnp.dot(a, b, preferred_element_type=F32)


def iota(shape, dim):
    return lax.broadcasted_iota(jnp.int32, shape, dim)


def kernel(dims, *refs):
    nz, npl, n_tp, tok_m, tok_a, width, ff, qw, kw = dims
    (
        routes_ref, routes_t_ref, weight_ref, egain_ref, again_ref, consts_ref, sink_ref,
        xm_hbm, wg_hbm, wu_hbm, wd_hbm, xa_hbm, wq_hbm, wk_hbm, wv_hbm, wo_hbm,
        attend_ref, expert_ref,
        xm, wg, wu, wd, xa, wqkv, wo,
        own, out_main, out_ext, grid_in, ext_in, part, rb1, sb, rb2, res_main, res_ext, back_main,
        back_ext, acc, normed, qs, kv, att, opart, ra1, sa, ra2,
        load_sem, disp_s, disp_r, ret_s, ret_r, ag_s, ag_r, rs_s, rs_r, halo_s, halo_r, ar_s, ar_r,
    ) = refs
    qd = width // n_tp
    half = qd // 2
    main_rows, ext_rows = npl * MAIN, npl * EXTRA
    chunk = main_rows + ext_rows
    eb = EXTRA * qd // 128
    n_ep = nz * npl
    ep = lax.axis_index("ep")
    tp = lax.axis_index("tp")
    z = ep // npl
    p = ep % npl
    right, left, opp = (tp + 1) % n_tp, (tp + n_tp - 1) % n_tp, (tp + 2) % n_tp
    after, before = (ep + 1) % n_ep, (ep + n_ep - 1) % n_ep

    barrier = pltpu.get_barrier_semaphore()

    def greet(k, carry):
        pl.semaphore_signal(barrier, inc=1, device_id={"ep": (ep + k) % n_ep}, device_id_type=MESH)
        return carry

    lax.fori_loop(1, n_ep, greet, 0)
    for side in (left, right):
        pl.semaphore_signal(barrier, inc=1, device_id={"tp": side}, device_id_type=MESH)

    loads = [
        (xm_hbm, xm), (xa_hbm, xa), (wq_hbm, wqkv.at[:, 0:qw]), (wk_hbm, wqkv.at[:, qw:qw + kw]),
        (wv_hbm, wqkv.at[:, qw + kw:qw + 2 * kw]), (wo_hbm, wo),
        (wg_hbm.at[0], wg), (wu_hbm.at[0], wu), (wd_hbm.at[0], wd),
    ]
    loads = [pltpu.make_async_copy(s, d, load_sem.at[i]) for i, (s, d) in enumerate(loads)]
    for copy in loads:
        copy.start()

    def slots(ids, axis):
        shape = (tok_m, n_ep) if axis == 0 else (n_ep, tok_m)
        experts = iota(shape, 1 - axis)
        hots = [(experts == r) for r in ids]
        lower = iota((tok_m, tok_m), 1 - axis) < iota((tok_m, tok_m), axis)
        tri = jnp.where(lower, 1.0, 0.0).astype(BF)
        result = []
        base = None
        for hot, r in zip(hots, ids):
            hot_b = jnp.where(hot, 1.0, 0.0).astype(BF)
            ranks = dot(tri, hot_b) if axis == 0 else dot(hot_b, tri)
            if base is not None:
                ranks = ranks + base
            else:
                base = jnp.sum(hot_b.astype(F32), axis=axis, keepdims=True)
            rank = jnp.sum(jnp.where(hot, ranks, 0.0), axis=1 - axis, keepdims=True).astype(jnp.int32)
            dz = lax.rem((r // npl) - z + nz, nz)
            index = jnp.where(2 * dz <= nz, jnp.maximum(2 * dz - 1, 0), 2 * (nz - dz))
            place = lax.rem(r, npl)
            inside = jnp.where(rank < MAIN, place * MAIN + rank, main_rows + place * EXTRA + rank - MAIN)
            result.append(index * chunk + inside)
        return result

    rows_t = routes_t_ref[...]
    slot_row = slots([rows_t[0:1, :], rows_t[1:2, :]], 1)
    rows_c = routes_ref[...]
    slot_col = slots([rows_c[:, 0:1], rows_c[:, 1:2]], 0)

    loads[0].wait()
    col0 = pl.multiple_of(tp * qd, 128)

    def norm_m(b, carry):
        rows = pl.ds(pl.multiple_of(b * 32, 32), 32)
        v = xm[rows, :].astype(F32)
        scale = lax.rsqrt(jnp.mean(v * v, axis=-1, keepdims=True) + epsilon)
        mine = xm[rows, pl.ds(col0, qd)].astype(F32)
        own[rows, :] = (mine * scale * egain_ref[:, pl.ds(col0, qd)]).astype(BF)
        return carry

    lax.fori_loop(0, tok_m // 32, norm_m, 0)
    pl.semaphore_wait(barrier, n_ep - 1 + 2)

    def delta(i):
        odd = lax.rem(i, 2)
        return odd * ((i + 1) // 2) - (1 - odd) * (i // 2)

    def fold_ext(e):
        total = jnp.zeros((npl * eb, 128), F32)
        r = iota((npl * eb, ext_rows), 0)
        c = iota((npl * eb, ext_rows), 1)
        src = (r // eb) * EXTRA + lax.rem(r, eb) // (qd // 128)
        for j in range(qd // 128):
            pick = jnp.where((src == c) & (lax.rem(r, qd // 128) == j), 1.0, 0.0).astype(BF)
            total = total + dot(pick, e[:, j * 128:(j + 1) * 128])
        return total.reshape(npl, eb, 128).astype(BF)

    def unfold_ext(x):
        flat = x.astype(F32).reshape(npl * eb, 128).astype(BF)
        r = iota((ext_rows, npl * eb), 0)
        c = iota((ext_rows, npl * eb), 1)
        want = (r // EXTRA) * eb + lax.rem(r, EXTRA) * (qd // 128)
        out = []
        for j in range(qd // 128):
            pick = jnp.where(want + j == c, 1.0, 0.0).astype(BF)
            out.append(dot(pick, flat).astype(BF))
        return out

    def exchange(i, main, ext, land_main, land_ext, sems, recv, dest_z):
        def body(k, carry):
            q = lax.rem(p + k, npl)
            dev = {"ep": dest_z * npl + q}
            pltpu.make_async_remote_copy(
                src_ref=main.at[i, pl.ds(pl.multiple_of(q * MAIN, MAIN), MAIN), :],
                dst_ref=land_main, send_sem=sems.at[i, 0], recv_sem=recv.at[i, 0],
                device_id=dev, device_id_type=MESH,
            ).start()
            pltpu.make_async_remote_copy(
                src_ref=ext.at[i, q], dst_ref=land_ext, send_sem=sems.at[i, 1],
                recv_sem=recv.at[i, 1], device_id=dev, device_id_type=MESH,
            ).start()
            return carry

        lax.fori_loop(1 - jnp.minimum(i, 1), npl, body, 0)

    def settle(i, main, ext, sems):
        for j, ref in ((0, main), (1, ext)):
            full = ref.at[i]
            few = ref.at[i, 0:(npl - 1) * MAIN, :] if j == 0 else ref.at[i, 0:npl - 1]

            @pl.when(i > 0)
            def _():
                pltpu.make_async_copy(full, full, sems.at[i, j]).wait()

            @pl.when(i == 0)
            def _():
                pltpu.make_async_copy(few, few, sems.at[i, j]).wait()

    my_main = pl.ds(pl.multiple_of(p * MAIN, MAIN), MAIN)
    my_cols = pl.ds(col0, qd)

    def dispatch(i, carry):
        slot = iota((chunk, tok_m), 0) + i * chunk
        hot = jnp.where((slot == slot_row[0]) | (slot == slot_row[1]), 1.0, 0.0).astype(BF)
        rows = dot(hot, own[...]).astype(BF)
        out_main[i] = rows[0:main_rows]
        out_ext[i] = fold_ext(rows[main_rows:])
        exchange(
            i, out_main, out_ext, grid_in.at[i, my_main, my_cols], ext_in.at[i, p],
            disp_s, disp_r, lax.rem(z + delta(i) + nz, nz),
        )
        return carry

    lax.fori_loop(0, nz, dispatch, 0)
    grid_in[0, my_main, my_cols] = out_main[0, my_main, :]
    ext_in[0, p] = out_ext[0, p]
    acc[...] = jnp.zeros_like(acc)

    def remote(src, dst, sems, recv, dev):
        return pltpu.make_async_remote_copy(
            src_ref=src, dst_ref=dst, send_sem=sems, recv_sem=recv, device_id={"tp": dev},
            device_id_type=MESH,
        )

    def cols(quarter, off, size):
        return pl.ds(pl.multiple_of(quarter * qd + off, 128), size)

    def ag_own(i):
        block = grid_in.at[i, :, my_cols]
        return [remote(block, block, ag_s.at[i, s], ag_r.at[i, s], d) for s, d in ((0, right), (1, left))]

    def ag_fwd(i):
        a = grid_in.at[i, :, cols(left, 0, half)]
        b = grid_in.at[i, :, cols(right, half, half)]
        return [
            remote(a, a, ag_s.at[i, 2], ag_r.at[i, 2], right),
            remote(b, b, ag_s.at[i, 3], ag_r.at[i, 3], left),
        ]

    def rs_one(i):
        return [
            remote(part.at[i, :, cols(opp, 0, half)], rb1.at[i, 0], rs_s.at[i, 0], rs_r.at[i, 0], right),
            remote(part.at[i, :, cols(opp, half, half)], rb1.at[i, 1], rs_s.at[i, 1], rs_r.at[i, 1], left),
        ]

    def rs_side(i):
        return [
            remote(part.at[i, :, cols(right, half, half)], rb2.at[i, 0, :, half:qd], rs_s.at[i, 2],
                   rs_r.at[i, 2], right),
            remote(part.at[i, :, cols(left, 0, half)], rb2.at[i, 1, :, 0:half], rs_s.at[i, 3],
                   rs_r.at[i, 3], left),
        ]

    def rs_two(i):
        return [
            remote(sb.at[i, 0], rb2.at[i, 0, :, 0:half], rs_s.at[i, 4], rs_r.at[i, 4], right),
            remote(sb.at[i, 1], rb2.at[i, 1, :, half:qd], rs_s.at[i, 5], rs_r.at[i, 5], left),
        ]

    quarter_rows = tok_a // n_tp
    hw = width // 2

    def rows_of(t):
        return pl.ds(pl.multiple_of(t * quarter_rows, quarter_rows), quarter_rows)

    def ar_one():
        return [
            remote(opart.at[rows_of(opp), 0:hw], ra1.at[0], ar_s.at[0], ar_r.at[0], right),
            remote(opart.at[rows_of(opp), hw:width], ra1.at[1], ar_s.at[1], ar_r.at[1], left),
        ]

    def ar_side():
        return [
            remote(opart.at[rows_of(right), hw:width], ra2.at[0, :, hw:width], ar_s.at[2], ar_r.at[2], right),
            remote(opart.at[rows_of(left), 0:hw], ra2.at[1, :, 0:hw], ar_s.at[3], ar_r.at[3], left),
        ]

    def ar_two():
        return [
            remote(sa.at[0], ra2.at[0, :, 0:hw], ar_s.at[4], ar_r.at[4], right),
            remote(sa.at[1], ra2.at[1, :, hw:width], ar_s.at[5], ar_r.at[5], left),
        ]

    def halo():
        out = []
        for s, (dev, src, dst) in enumerate((
            (after, kv.at[tok_a:tok_a + WINDOW, :], kv.at[0:WINDOW, :]),
            (before, kv.at[WINDOW:2 * WINDOW, :], kv.at[tok_a + WINDOW:tok_a + 2 * WINDOW, :]),
        )):
            out.append(pltpu.make_async_remote_copy(
                src_ref=src, dst_ref=dst, send_sem=halo_s.at[s], recv_sem=halo_r.at[s],
                device_id={"ep": dev}, device_id_type=MESH,
            ))
        return out

    def start(copies):
        for c in copies:
            c.start()

    def arrived(copies):
        for c in copies:
            c.wait_recv()

    def sent(copies):
        for c in copies:
            c.wait_send()

    half_dim = HEAD_DIM // 2

    def qkv_all():
        for copy in loads[1:5]:
            copy.wait()
        inv = consts_ref[2:3, :]
        lane = lax.rem(iota((GRID_W, 128), 1), half_dim)
        is_row = lane < half_dim // 2
        col_ang = iota((GRID_W, 128), 0).astype(F32) * inv
        groups = tok_a // GRID_W
        row_ang = (iota((groups, 128), 0) + ep * groups).astype(F32) * inv
        col_cos, col_sin = jnp.cos(col_ang), jnp.sin(col_ang)
        row_cos, row_sin = jnp.cos(row_ang), jnp.sin(row_ang)
        first = lax.rem(iota((1, 128), 1), HEAD_DIM) < half_dim
        sign = jnp.where(first, -1.0, 1.0)
        tables = []
        for g in range(groups):
            c = jnp.where(is_row, row_cos[g:g + 1, :], col_cos)
            s = jnp.where(is_row, row_sin[g:g + 1, :], col_sin) * sign
            tables.append((c, s))
        ones = jnp.where(iota((128, 128), 0) // HEAD_DIM == iota((128, 128), 1) // HEAD_DIM, 1.0, 0.0).astype(BF)

        def rotated(v, gain, c, s):
            sq = v * v
            hi = sq.astype(BF)
            lo = (sq - hi.astype(F32)).astype(BF)
            mean = (dot(hi, ones) + dot(lo, ones)) * (1.0 / HEAD_DIM)
            scaled = v * lax.rsqrt(mean + epsilon) * gain
            other = jnp.where(first, pltpu.roll(scaled, 128 - half_dim, 1), pltpu.roll(scaled, half_dim, 1))
            return (scaled * c + other * s).astype(BF)

        blk = 128
        for b in range(tok_a // blk):
            def norm_a(j, carry):
                rows = pl.ds(pl.multiple_of(b * blk + j * 32, 32), 32)
                v = xa[rows, :].astype(F32)
                scale = lax.rsqrt(jnp.mean(v * v, axis=-1, keepdims=True) + epsilon)
                normed[rows, :] = (v * scale * again_ref[...]).astype(BF)
                return carry

            lax.fori_loop(0, blk // 32, norm_a, 0)
            rows = slice(b * blk, (b + 1) * blk)
            proj = dot(normed[rows, :], wqkv[...])
            per = blk // GRID_W
            c = jnp.concatenate([tables[b * per + j][0] for j in range(per)], axis=0)
            s = jnp.concatenate([tables[b * per + j][1] for j in range(per)], axis=0)
            for j in range(qw // 128):
                sl = slice(j * 128, (j + 1) * 128)
                qs[rows, sl] = rotated(proj[:, sl], consts_ref[0:1, :], c, s)
            dst = slice(WINDOW + b * blk, WINDOW + (b + 1) * blk)
            kv[dst, 0:kw] = rotated(proj[:, qw:qw + kw], consts_ref[1:2, :], c, s)
            kv[dst, kw:2 * kw] = proj[:, qw + kw:qw + 2 * kw].astype(BF)

    kv_local = kw // HEAD_DIM
    group = qw // kw

    def attend_all():
        loads[5].wait()
        total_len = tok_a * n_ep
        span = 3 * WINDOW

        def block(b, carry):
            row0 = pl.multiple_of(b * WINDOW, WINDOW)
            q_rows = pl.ds(row0, WINDOW)
            k_rows = pl.ds(row0, span)
            gap = iota((WINDOW, span), 1) - iota((WINDOW, span), 0)
            pos = ep * tok_a - WINDOW + row0 + iota((WINDOW, span), 1)
            valid = (gap >= 0) & (gap <= 2 * WINDOW) & (pos >= 0) & (pos < total_len)
            for h in range(kv_local):
                keys = kv[k_rows, h * HEAD_DIM:(h + 1) * HEAD_DIM]
                vals = kv[k_rows, kw + h * HEAD_DIM:kw + (h + 1) * HEAD_DIM]
                for g in range(group):
                    head = h * group + g
                    lanes = slice(head * HEAD_DIM, (head + 1) * HEAD_DIM)
                    q = qs[q_rows, lanes]
                    s = lax.dot_general(q, keys, (((1,), (1,)), ((), ())), preferred_element_type=F32)
                    s = jnp.where(valid, s * HEAD_DIM ** (-0.5), -1e30)
                    sink = sink_ref[head]
                    peak = jnp.maximum(jnp.max(s, axis=-1, keepdims=True), sink)
                    w = jnp.exp(s - peak)
                    denom = jnp.sum(w, axis=-1, keepdims=True) + jnp.exp(sink - peak)
                    probs = (w * (1.0 / denom)).astype(BF)
                    att[:, lanes] = dot(probs, vals).astype(BF)
            opart[q_rows, :] = dot(att[...], wo[...]).astype(BF)
            return carry

        lax.fori_loop(0, tok_a // WINDOW, block, 0)

    def tick(i, carry):
        @pl.when(i < nz)
        def _():
            settle(i, out_main, ext_in, disp_r)
            e = unfold_ext(ext_in[i])
            for j, piece in enumerate(e):
                grid_in[i, main_rows:chunk, cols(tp, j * 128, 128)] = piece
            start(ag_own(i))

        @pl.when((i >= 1) & (i < nz + 1))
        def _():
            arrived(ag_own(i - 1))
            start(ag_fwd(i - 1))

        @pl.when(i == 0)
        def _():
            qkv_all()
            start(halo())

        @pl.when((i >= 2) & (i < nz + 2))
        def _():
            c = i - 2

            @pl.when(c == 0)
            def _():
                for copy in loads[6:9]:
                    copy.wait()

            arrived(ag_fwd(c))
            x = grid_in[c]
            g = dot(x, wg[...])
            u = dot(x, wu[...])
            hidden = (g / (1.0 + jnp.exp(-g)) * u).astype(BF)
            part[c] = dot(hidden, wd[...]).astype(BF)
            start(rs_one(c))
            start(rs_side(c))

        @pl.when((i >= 3) & (i < nz + 3))
        def _():
            c = i - 3
            arrived(rs_one(c))
            for s, (quarter, off) in enumerate(((right, 0), (left, half))):
                mine = part[c, :, cols(quarter, off, half)].astype(F32)
                sb[c, s] = (mine + rb1[c, s].astype(F32)).astype(BF)
            start(rs_two(c))

        @pl.when((i >= 4) & (i < nz + 4))
        def _():
            c = i - 4
            arrived(rs_side(c))
            arrived(rs_two(c))
            total = part[c, :, my_cols].astype(F32) + rb2[c, 0].astype(F32) + rb2[c, 1].astype(F32)
            total = total.astype(BF)
            res_main[c] = total[0:main_rows]
            res_ext[c] = fold_ext(total[main_rows:])
            exchange(
                c, res_main, res_ext, back_main.at[c, my_main, :], back_ext.at[c, p],
                ret_s, ret_r, lax.rem(z - delta(c) + nz, nz),
            )

            @pl.when(c == 0)
            def _():
                back_main[0, my_main, :] = res_main[0, my_main, :]
                back_ext[0, p] = res_ext[0, p]

        @pl.when(i == 1)
        def _():
            arrived(halo())
            attend_all()
            start(ar_one())
            start(ar_side())

        @pl.when(i == 2)
        def _():
            arrived(ar_one())
            for s, (t, off) in enumerate(((right, 0), (left, hw))):
                mine = opart[rows_of(t), off:off + hw].astype(F32)
                sa[s] = (mine + ra1[s].astype(F32)).astype(BF)
            start(ar_two())

        @pl.when(i == 4)
        def _():
            arrived(ar_side())
            arrived(ar_two())
            total = opart[rows_of(tp), :].astype(F32) + ra2[0].astype(F32) + ra2[1].astype(F32)
            attend_ref[...] = total.astype(BF)

        @pl.when(i >= 5)
        def _():
            c = i - 5
            settle(c, back_main, back_ext, ret_r)
            e = unfold_ext(back_ext[c])
            slot = iota((tok_m, chunk), 1) + c * chunk
            for k in range(2):
                hot = jnp.where(slot == slot_col[k], 1.0, 0.0).astype(BF)
                acc[k] += dot(hot[:, 0:main_rows], back_main[c])
                for j, piece in enumerate(e):
                    sl = slice(j * 128, (j + 1) * 128)
                    acc[k, :, sl] += dot(hot[:, main_rows:], piece)

        return carry

    lax.fori_loop(0, nz + 5, tick, 0)
    weights = weight_ref[...]
    expert_ref[...] = (acc[0] * weights[:, 0:1] + acc[1] * weights[:, 1:2]).astype(BF)

    def drain(i, carry):
        settle(i, out_main, out_ext, disp_s)
        settle(i, res_main, res_ext, ret_s)
        for stage in (ag_own, ag_fwd, rs_one, rs_side, rs_two):
            sent(stage(i))
        return carry

    lax.fori_loop(0, nz, drain, 0)
    for stage in (halo, ar_one, ar_side, ar_two):
        sent(stage())


def fused(dims, *args):
    nz, npl, n_tp, tok_m, tok_a, width, ff, qw, kw = dims
    qd = width // n_tp
    half = qd // 2
    chunk = npl * (MAIN + EXTRA)
    eb = EXTRA * qd // 128
    hw = width // 2
    qr = tok_a // n_tp
    vm = pltpu.VMEM
    dma = pltpu.SemaphoreType.DMA
    any_spec = pl.BlockSpec(memory_space=pl.ANY)
    vmem_spec = pl.BlockSpec(memory_space=pltpu.VMEM)
    smem_spec = pl.BlockSpec(memory_space=pltpu.SMEM)
    return pl.pallas_call(
        functools.partial(kernel, dims),
        out_shape=(
            jax.ShapeDtypeStruct((qr, width), BF),
            jax.ShapeDtypeStruct((tok_m, qd), BF),
        ),
        in_specs=[vmem_spec] * 6 + [smem_spec] + [any_spec] * 9,
        out_specs=(vmem_spec, vmem_spec),
        scratch_shapes=[
            vm((tok_m, width), BF), vm((width, ff), BF), vm((width, ff), BF), vm((ff, width), BF),
            vm((tok_a, width), BF), vm((width, qw + 2 * kw), BF), vm((qw, width), BF),
            vm((tok_m, qd), BF),
            vm((nz, npl * MAIN, qd), BF), vm((nz, npl, eb, 128), BF),
            vm((nz, chunk, width), BF), vm((nz, npl, eb, 128), BF),
            vm((nz, chunk, width), BF),
            vm((nz, 2, chunk, half), BF), vm((nz, 2, chunk, half), BF), vm((nz, 2, chunk, qd), BF),
            vm((nz, npl * MAIN, qd), BF), vm((nz, npl, eb, 128), BF),
            vm((nz, npl * MAIN, qd), BF), vm((nz, npl, eb, 128), BF),
            vm((2, tok_m, qd), F32),
            vm((tok_a, width), BF), vm((tok_a, qw), BF), vm((tok_a + 2 * WINDOW, 2 * kw), BF),
            vm((WINDOW, qw), BF), vm((tok_a, width), BF),
            vm((2, qr, hw), BF), vm((2, qr, hw), BF), vm((2, qr, width), BF),
            dma((9,)), dma((nz, 2)), dma((nz, 2)), dma((nz, 2)), dma((nz, 2)),
            dma((nz, 4)), dma((nz, 4)), dma((nz, 6)), dma((nz, 6)),
            dma((2,)), dma((2,)), dma((6,)), dma((6,)),
        ],
        compiler_params=pltpu.CompilerParams(
            collective_id=0, has_side_effects=True, vmem_limit_bytes=60 * 1024 * 1024
        ),
        name="fused_layer",
    )(*args)


def per_device(
    planes,
    x_attend, attend_gain, w_query, w_key, w_value, query_gain, key_gain, sink_logit, w_output,
    x_experts, expert_gain, routes, group_prob, expert_prob, w_gate, w_up, w_down,
):
    n_ep, n_tp = lax.axis_size("ep"), lax.axis_size("tp")
    tok_a, width = x_attend.shape
    dims = (
        planes, n_ep // planes, n_tp, x_experts.shape[0], tok_a, width, w_gate.shape[2],
        w_query.shape[1], w_key.shape[1],
    )
    half_dim = HEAD_DIM // 2
    inverse = rope_base ** (-jnp.arange(0, half_dim, 2, dtype=jnp.float32) / half_dim)
    consts = jnp.stack([
        jnp.tile(query_gain, 2), jnp.tile(key_gain, 2), jnp.tile(inverse, 256 // half_dim),
    ])
    weights = group_prob[:, None] * expert_prob / jnp.sum(expert_prob, axis=1, keepdims=True)
    return fused(
        dims, routes, routes.T, weights, expert_gain[None, :], attend_gain[None, :], consts,
        sink_logit, x_experts, w_gate, w_up, w_down, x_attend, w_query, w_key, w_value, w_output,
    )


def solution(mesh, planes=8):
    placed = (
        P("ep", None), P(), P(None, "tp"), P(None, "tp"), P(None, "tp"), P(), P(), P("tp"),
        P("tp", None), P("ep", None), P(), P("ep", None), P("ep"), P("ep", None),
        P("ep", None, "tp"), P("ep", None, "tp"), P("ep", "tp", None),
    )
    return jax.shard_map(
        functools.partial(per_device, planes),
        mesh=mesh,
        in_specs=placed,
        out_specs=(P(("ep", "tp"), None), P("ep", "tp")),
        check_vma=False,
    )
```

```python
import functools

import jax
import jax.numpy as jnp
import numpy as np
from jax import lax
from jax.experimental import pallas as pl
from jax.experimental.pallas import tpu as pltpu
from jax.sharding import PartitionSpec as P

HEAD_DIM = 64
WINDOW = 128
GRID_W = 64
MAIN = 16
EXTRA = 2
FIRST_ATT = 3
LAG = 4

epsilon = 1e-06
rope_base = 10000.0

BF = jnp.bfloat16
F32 = jnp.float32
MESH = pl.DeviceIdType.MESH


def dot(a, b):
    return jnp.dot(a, b, preferred_element_type=F32)


def iota(shape, dim):
    return lax.broadcasted_iota(jnp.int32, shape, dim)


ORDERS = {8: ((0, 2, 6, 5, 4, 3, 7, 1), 5), 4: ((0, 2, 3, 1), 1), 2: ((0, 1), 1)}


def kernel(dims, *refs):
    nz, npl, n_tp, tok_m, tok_a, width, ff, qw, kw = dims
    (
        routes_ref, prob_ref, gprob_ref, egain_ref, again_ref, qgain_ref, kgain_ref, inv_ref, sink_ref,
        xm_hbm, wg_hbm, wu_hbm, wd_hbm, xa_hbm, wq_hbm, wk_hbm, wv_hbm, wo_hbm,
        attend_ref, expert_ref,
        xm, wg, wu, wd, xa, wqkv, wo,
        own, out_main, out_ext, full_main, full_ext, grid_in, ext_in, fext_in, part, rb1, sb, rb2,
        res_main, res_ext, back_main, back_ext, acc, normed, qs, kv, att, att_all,
        load_sem, disp_s, disp_r, ret_s, ret_r, ag_s, ag_r, rs_s, rs_r, halo_s, halo_r, wo_s, wo_r, at_s, at_r,
    ) = refs
    order, n_ag = ORDERS[nz]
    qd = width // n_tp
    half = qd // 2
    main_rows, ext_rows = npl * MAIN, npl * EXTRA
    chunk = main_rows + ext_rows
    eb = EXTRA * qd // 128
    n_ep = nz * npl
    ep = lax.axis_index("ep")
    tp = lax.axis_index("tp")
    z = ep // npl
    p = ep % npl
    nx = npl // 2
    xc, core = p // 2, p % 2
    right, left, opp = (tp + 1) % n_tp, (tp + n_tp - 1) % n_tp, (tp + 2) % n_tp
    after, before = (ep + 1) % n_ep, (ep + n_ep - 1) % n_ep

    barrier = pltpu.get_barrier_semaphore()

    def greet(k, carry):
        pl.semaphore_signal(barrier, inc=1, device_id={"ep": (ep + k) % n_ep}, device_id_type=MESH)
        return carry

    loads = [
        (xm_hbm, xm), (wo_hbm, wo.at[tp]), (xa_hbm, xa), (wq_hbm, wqkv.at[:, 0:qw]), (wk_hbm, wqkv.at[:, qw:qw + kw]),
        (wv_hbm, wqkv.at[:, qw + kw:qw + 2 * kw]),
        (wg_hbm.at[0], wg), (wu_hbm.at[0], wu), (wd_hbm.at[0], wd),
    ]
    loads = [pltpu.make_async_copy(s, d, load_sem.at[i]) for i, (s, d) in enumerate(loads)]
    loads[0].start()
    lax.fori_loop(1, n_ep, greet, 0)
    for side in (left, right, opp):
        pl.semaphore_signal(barrier, inc=1, device_id={"tp": side}, device_id_type=MESH)
    for copy in loads[1:]:
        copy.start()

    ids = [routes_ref[k:k + 1, :] for k in range(2)]
    experts = iota((n_ep, tok_m), 0)
    tri = jnp.where(iota((tok_m, tok_m), 0) < iota((tok_m, tok_m), 1), 1.0, 0.0).astype(BF)
    slot_row = []
    base = None
    for r in ids:
        hot = experts == r
        hot_b = jnp.where(hot, 1.0, 0.0).astype(BF)
        ranks = dot(hot_b, tri)
        if base is None:
            base = jnp.sum(hot_b.astype(F32), axis=1, keepdims=True)
        else:
            ranks = ranks + base
        rank = jnp.sum(jnp.where(hot, ranks, 0.0), axis=0, keepdims=True).astype(jnp.int32)
        dz = lax.rem((r // npl) - z + nz, nz)
        index = jnp.zeros_like(r)
        for i, d in enumerate(order):
            index = jnp.where(dz == d, i, index)
        place = lax.rem(r, npl)
        inside = jnp.where(rank < MAIN, place * MAIN + rank, main_rows + place * EXTRA + rank - MAIN)
        slot_row.append(index * chunk + inside)

    loads[0].wait()
    col0 = pl.multiple_of(tp * qd, 128)

    def norm_m(b, carry):
        rows = pl.ds(pl.multiple_of(b * 32, 32), 32)
        v = xm[rows, :].astype(F32)
        scale = lax.rsqrt(jnp.mean(v * v, axis=-1, keepdims=True) + epsilon)
        own[rows, :] = (v * scale * egain_ref[...]).astype(BF)
        return carry

    lax.fori_loop(0, tok_m // 32, norm_m, 0)
    loads[1].wait()
    pl.semaphore_wait(barrier, n_ep - 1 + 3)

    def delta(i):
        code = sum(d << (3 * k) for k, d in enumerate(order))
        return lax.rem(lax.shift_right_logical(jnp.int32(code), 3 * i), 8)

    def fold_ext(e, blocks):
        n = npl * EXTRA * blocks
        total = jnp.zeros((n, 128), F32)
        r = iota((n, ext_rows), 0)
        c = iota((n, ext_rows), 1)
        for j in range(blocks):
            pick = jnp.where((r // blocks == c) & (lax.rem(r, blocks) == j), 1.0, 0.0).astype(BF)
            total = total + dot(pick, e[:, j * 128:(j + 1) * 128])
        return total.reshape(npl, EXTRA * blocks, 128).astype(BF)

    def unfold_ext(x, blocks):
        n = npl * EXTRA * blocks
        flat = x.astype(F32).reshape(n, 128).astype(BF)
        r = iota((ext_rows, n), 0)
        c = iota((ext_rows, n), 1)
        out = []
        for j in range(blocks):
            pick = jnp.where(r * blocks + j == c, 1.0, 0.0).astype(BF)
            out.append(dot(pick, flat).astype(BF))
        return out

    def exchange(i, m, main, ext, land_main, land_ext, sems, recv, dest_z):
        def body(k, carry):
            q = lax.rem(p + k, npl)
            dev = {"ep": dest_z * npl + q}
            pltpu.make_async_remote_copy(
                src_ref=main.at[m, pl.ds(pl.multiple_of(q * MAIN, MAIN), MAIN), :],
                dst_ref=land_main, send_sem=sems.at[i, 0], recv_sem=recv.at[i, 0],
                device_id=dev, device_id_type=MESH,
            ).start()
            pltpu.make_async_remote_copy(
                src_ref=ext.at[m, q], dst_ref=land_ext, send_sem=sems.at[i, 1],
                recv_sem=recv.at[i, 1], device_id=dev, device_id_type=MESH,
            ).start()
            return carry

        lax.fori_loop(1 - jnp.minimum(i, 1), npl, body, 0)

    def settle(i, m, main, ext, sems):
        for j, ref in ((0, main), (1, ext)):
            full = ref.at[m]
            few = ref.at[m, 0:(npl - 1) * MAIN, :] if j == 0 else ref.at[m, 0:npl - 1]

            @pl.when(i > 0)
            def _():
                pltpu.make_async_copy(full, full, sems.at[i, j]).wait()

            @pl.when(i == 0)
            def _():
                pltpu.make_async_copy(few, few, sems.at[i, j]).wait()

    my_main = pl.ds(pl.multiple_of(p * MAIN, MAIN), MAIN)
    my_cols = pl.ds(col0, qd)
    lanes_q, lanes_f = qd // 128, width // 128

    def hot_rows(i):
        slot = iota((chunk, tok_m), 0) + i * chunk
        return jnp.where((slot == slot_row[0]) | (slot == slot_row[1]), 1.0, 0.0).astype(BF)

    def full_of(i):
        return jnp.maximum(i - n_ag, 0)

    def dispatch(i, carry):
        rows = dot(hot_rows(i), own[:, my_cols]).astype(BF)
        out_main[i] = rows[0:main_rows]
        out_ext[i] = fold_ext(rows[main_rows:], lanes_q)
        exchange(
            i, i, out_main, out_ext, grid_in.at[i, my_main, my_cols], ext_in.at[i, p],
            disp_s, disp_r, lax.rem(z + delta(i), nz),
        )
        return carry

    def dispatch_full(i, carry):
        d = full_of(i)
        rows = dot(hot_rows(i), own[...]).astype(BF)
        full_main[d] = rows[0:main_rows]
        full_ext[d] = fold_ext(rows[main_rows:], lanes_f)
        exchange(
            i, d, full_main, full_ext, grid_in.at[i, my_main, :], fext_in.at[d, p],
            disp_s, disp_r, lax.rem(z + delta(i), nz),
        )
        return carry

    def start(copies):
        for c in copies:
            c.start()

    def arrived(copies):
        for c in copies:
            c.wait_recv()

    def sent(copies):
        for c in copies:
            c.wait_send()

    def remote(src, dst, sems, recv, dev):
        return pltpu.make_async_remote_copy(
            src_ref=src, dst_ref=dst, send_sem=sems, recv_sem=recv, device_id=dev,
            device_id_type=MESH,
        )

    hw = width // 2
    hrows = qw // 2
    srows = hrows // nx
    my_slice = pl.ds(pl.multiple_of(core * hrows + xc * srows, 16), srows)
    my_half = pl.ds(pl.multiple_of(core * hrows, 16), hrows)

    def wo_own():
        ref = wo.at[tp, my_slice, :]
        return [remote(ref, ref, wo_s.at[k], wo_r.at[k], {"tp": d}) for k, d in ((0, right), (1, left))]

    def wo_fwd():
        a = wo.at[left, my_slice, 0:hw]
        b = wo.at[right, my_slice, hw:width]
        return [
            remote(a, a, wo_s.at[2], wo_r.at[2], {"tp": right}),
            remote(b, b, wo_s.at[3], wo_r.at[3], {"tp": left}),
        ]

    def wo_along():
        out = []
        for k in range(1, nx):
            dev = {"ep": z * npl + lax.rem(xc + k, nx) * 2 + core}
            for shard in (right, left, opp):
                ref = wo.at[shard, my_slice, :]
                out.append(remote(ref, ref, wo_s.at[4], wo_r.at[4], dev))
        return out

    def wo_along_done(sems):
        if nx > 1:
            ref = wo.at[0:3, 0:(nx - 1) * srows, :]
            pltpu.make_async_copy(ref, ref, sems.at[4]).wait()

    def wo_core():
        out = []
        for shard in (right, left, opp):
            ref = wo.at[shard, my_half, :]
            out.append(remote(ref, ref, wo_s.at[5], wo_r.at[5], {"ep": z * npl + xc * 2 + 1 - core}))
        return out

    def wo_core_done(sems):
        ref = wo.at[0:3, 0:hrows, :]
        pltpu.make_async_copy(ref, ref, sems.at[5]).wait()

    start(wo_own())
    lax.fori_loop(1, min(3, n_ag + 1), dispatch, 0)
    dispatch_full(0, 0)
    lax.fori_loop(min(3, n_ag + 1), n_ag + 1, dispatch, 0)
    lax.fori_loop(n_ag + 1, nz, dispatch_full, 0)
    grid_in[0, my_main, :] = full_main[0, my_main, :]
    fext_in[0, p] = full_ext[0, p]
    acc[...] = jnp.zeros_like(acc)

    eye = iota((tok_m, tok_m), 0) == iota((tok_m, tok_m), 1)

    def column(row):
        return jnp.sum(jnp.where(eye, row, 0.0), axis=1, keepdims=True)

    slot_col = [column(r.astype(F32)).astype(jnp.int32) for r in slot_row]
    probs = [prob_ref[k:k + 1, :] for k in range(2)]
    weight_col = [column(gprob_ref[...] * q / (probs[0] + probs[1])) for q in probs]

    def cols(quarter, off, size):
        return pl.ds(pl.multiple_of(quarter * qd + off, 128), size)

    def ag_own(i):
        block = grid_in.at[i, :, my_cols]
        return [
            remote(block, block, ag_s.at[i, s], ag_r.at[i, s], {"tp": d}) for s, d in ((0, right), (1, left))
        ]

    def ag_fwd(i):
        a = grid_in.at[i, :, cols(left, 0, half)]
        b = grid_in.at[i, :, cols(right, half, half)]
        return [
            remote(a, a, ag_s.at[i, 2], ag_r.at[i, 2], {"tp": right}),
            remote(b, b, ag_s.at[i, 3], ag_r.at[i, 3], {"tp": left}),
        ]

    def rs_one(i):
        a = part.at[i, :, cols(opp, 0, half)]
        b = part.at[i, :, cols(opp, half, half)]
        return [
            remote(a, rb1.at[i, 0], rs_s.at[i, 0], rs_r.at[i, 0], {"tp": right}),
            remote(b, rb1.at[i, 1], rs_s.at[i, 1], rs_r.at[i, 1], {"tp": left}),
        ]

    def rs_side(i):
        a = part.at[i, :, cols(right, half, half)]
        b = part.at[i, :, cols(left, 0, half)]
        return [
            remote(a, rb2.at[i, 0, :, half:qd], rs_s.at[i, 2], rs_r.at[i, 2], {"tp": right}),
            remote(b, rb2.at[i, 1, :, 0:half], rs_s.at[i, 3], rs_r.at[i, 3], {"tp": left}),
        ]

    def rs_two(i):
        return [
            remote(sb.at[i, 0], rb2.at[i, 0, :, 0:half], rs_s.at[i, 4], rs_r.at[i, 4], {"tp": right}),
            remote(sb.at[i, 1], rb2.at[i, 1, :, half:qd], rs_s.at[i, 5], rs_r.at[i, 5], {"tp": left}),
        ]

    quarter_rows = tok_a // n_tp

    def rows_of(t):
        return pl.ds(pl.multiple_of(t * quarter_rows, quarter_rows), quarter_rows)

    my_heads = pl.ds(pl.multiple_of(tp * qw, 128), qw)

    def att_send():
        return [
            remote(att.at[rows_of(d), :], att_all.at[:, my_heads], at_s.at[k], at_r.at[k], {"tp": d})
            for k, d in enumerate((right, left, opp))
        ]

    def halo():
        low, high = kv.at[0:WINDOW, :], kv.at[tok_a + WINDOW:tok_a + 2 * WINDOW, :]
        return [
            remote(kv.at[tok_a:tok_a + WINDOW, :], low, halo_s.at[0], halo_r.at[0], {"ep": after}),
            remote(kv.at[WINDOW:2 * WINDOW, :], high, halo_s.at[1], halo_r.at[1], {"ep": before}),
        ]

    half_dim = HEAD_DIM // 2

    def qkv_all():
        for copy in loads[2:6]:
            copy.wait()
        inv = inv_ref[...]
        q_gain = jnp.concatenate([qgain_ref[...]] * 2, axis=1)
        k_gain = jnp.concatenate([kgain_ref[...]] * 2, axis=1)
        lane = lax.rem(iota((GRID_W, 128), 1), half_dim)
        is_row = lane < half_dim // 2
        col_ang = iota((GRID_W, 128), 0).astype(F32) * inv
        groups = tok_a // GRID_W
        row_ang = (iota((groups, 128), 0) + ep * groups).astype(F32) * inv
        col_cos, col_sin = jnp.cos(col_ang), jnp.sin(col_ang)
        row_cos, row_sin = jnp.cos(row_ang), jnp.sin(row_ang)
        first = lax.rem(iota((1, 128), 1), HEAD_DIM) < half_dim
        sign = jnp.where(first, -1.0, 1.0)
        tables = []
        for g in range(groups):
            c = jnp.where(is_row, row_cos[g:g + 1, :], col_cos)
            s = jnp.where(is_row, row_sin[g:g + 1, :], col_sin) * sign
            tables.append((c, s))
        ones = jnp.where(iota((128, 128), 0) // HEAD_DIM == iota((128, 128), 1) // HEAD_DIM, 1.0, 0.0).astype(BF)

        def rotated(v, gain, c, s):
            sq = v * v
            hi = sq.astype(BF)
            lo = (sq - hi.astype(F32)).astype(BF)
            mean = (dot(hi, ones) + dot(lo, ones)) * (1.0 / HEAD_DIM)
            scaled = v * lax.rsqrt(mean + epsilon) * gain
            other = jnp.where(first, pltpu.roll(scaled, 128 - half_dim, 1), pltpu.roll(scaled, half_dim, 1))
            return (scaled * c + other * s).astype(BF)

        blk = 128
        for b in range(tok_a // blk):
            def norm_a(j, carry):
                rows = pl.ds(pl.multiple_of(b * blk + j * 32, 32), 32)
                v = xa[rows, :].astype(F32)
                scale = lax.rsqrt(jnp.mean(v * v, axis=-1, keepdims=True) + epsilon)
                normed[rows, :] = (v * scale * again_ref[...]).astype(BF)
                return carry

            lax.fori_loop(0, blk // 32, norm_a, 0)
            rows = slice(b * blk, (b + 1) * blk)
            proj = dot(normed[rows, :], wqkv[...])
            per = blk // GRID_W
            c = jnp.concatenate([tables[b * per + j][0] for j in range(per)], axis=0)
            s = jnp.concatenate([tables[b * per + j][1] for j in range(per)], axis=0)
            for j in range(qw // 128):
                sl = slice(j * 128, (j + 1) * 128)
                qs[rows, sl] = rotated(proj[:, sl], q_gain, c, s)
            dst = slice(WINDOW + b * blk, WINDOW + (b + 1) * blk)
            kv[dst, 0:kw] = rotated(proj[:, qw:qw + kw], k_gain, c, s)
            kv[dst, kw:2 * kw] = proj[:, qw + kw:qw + 2 * kw].astype(BF)

    kv_local = kw // HEAD_DIM
    group = qw // kw
    total_len = tok_a * n_ep
    span = 3 * WINDOW

    def attend(b):
        row0 = pl.multiple_of(b * WINDOW, WINDOW)
        q_rows = pl.ds(row0, WINDOW)
        k_rows = pl.ds(row0, span)
        gap = iota((WINDOW, span), 1) - iota((WINDOW, span), 0)
        pos = ep * tok_a - WINDOW + row0 + iota((WINDOW, span), 1)
        valid = (gap >= 0) & (gap <= 2 * WINDOW) & (pos >= 0) & (pos < total_len)
        for h in range(kv_local):
            keys = kv[k_rows, h * HEAD_DIM:(h + 1) * HEAD_DIM]
            vals = kv[k_rows, kw + h * HEAD_DIM:kw + (h + 1) * HEAD_DIM]
            for g in range(group):
                head = h * group + g
                lanes = slice(head * HEAD_DIM, (head + 1) * HEAD_DIM)
                q = qs[q_rows, lanes]
                s = lax.dot_general(q, keys, (((1,), (1,)), ((), ())), preferred_element_type=F32)
                s = jnp.where(valid, s * HEAD_DIM ** (-0.5), -1e30)
                sink = sink_ref[head]
                peak = jnp.maximum(jnp.max(s, axis=-1, keepdims=True), sink)
                w = jnp.exp(s - peak)
                denom = jnp.sum(w, axis=-1, keepdims=True) + jnp.exp(sink - peak)
                weights = (w * (1.0 / denom)).astype(BF)
                att[q_rows, lanes] = dot(weights, vals).astype(BF)

    n_blocks = tok_a // WINDOW

    qkv_all()
    start(halo())

    def tick(i, carry):
        @pl.when(i < n_ag)
        def _():
            c = i + 1
            settle(c, c, out_main, ext_in, disp_r)
            for j, piece in enumerate(unfold_ext(ext_in[c], lanes_q)):
                grid_in[c, main_rows:chunk, cols(tp, j * 128, 128)] = piece
            start(ag_own(c))

        @pl.when(i == 0)
        def _():
            arrived(wo_own())
            start(wo_fwd())

        @pl.when((i >= 1) & (i < n_ag + 1))
        def _():
            arrived(ag_own(i))
            start(ag_fwd(i))

        @pl.when(i == 1)
        def _():
            arrived(wo_fwd())
            start(wo_along())

        @pl.when((i >= 1) & (i < nz + 1))
        def _():
            c = i - 1

            @pl.when(c == 0)
            def _():
                for copy in loads[6:9]:
                    copy.wait()

            direct = (c == 0) | (c > n_ag)

            @pl.when(direct)
            def _():
                d = full_of(c)
                settle(c, d, full_main, fext_in, disp_r)
                for j, piece in enumerate(unfold_ext(fext_in[d], lanes_f)):
                    grid_in[c, main_rows:chunk, j * 128:(j + 1) * 128] = piece

            @pl.when(jnp.logical_not(direct))
            def _():
                arrived(ag_fwd(c))

            x = grid_in[c]
            g = dot(x, wg[...])
            u = dot(x, wu[...])
            hidden = (g / (1.0 + jnp.exp(-g)) * u).astype(BF)
            part[c] = dot(hidden, wd[...]).astype(BF)
            start(rs_one(c))
            start(rs_side(c))

        @pl.when((i >= 2) & (i < nz + 2))
        def _():
            c = i - 2
            arrived(rs_one(c))
            for s, (quarter, off) in enumerate(((right, 0), (left, half))):
                mine = part[c, :, cols(quarter, off, half)].astype(F32)
                sb[c, s] = (mine + rb1[c, s].astype(F32)).astype(BF)
            start(rs_two(c))

        @pl.when((i >= 3) & (i < nz + 3))
        def _():
            c = i - 3
            arrived(rs_side(c))
            arrived(rs_two(c))
            total = part[c, :, my_cols].astype(F32) + rb2[c, 0].astype(F32) + rb2[c, 1].astype(F32)
            total = total.astype(BF)
            res_main[c] = total[0:main_rows]
            res_ext[c] = fold_ext(total[main_rows:], lanes_q)
            exchange(
                c, c, res_main, res_ext, back_main.at[c, my_main, :], back_ext.at[c, p],
                ret_s, ret_r, lax.rem(z - delta(c) + nz, nz),
            )

            @pl.when(c == 0)
            def _():
                back_main[0, my_main, :] = res_main[0, my_main, :]
                back_ext[0, p] = res_ext[0, p]

        @pl.when(i == FIRST_ATT)
        def _():
            arrived(halo())

        @pl.when((i >= FIRST_ATT) & (i < FIRST_ATT + n_blocks))
        def _():
            attend(i - FIRST_ATT)

        last_att = FIRST_ATT + n_blocks - 1

        @pl.when(i == last_att)
        def _():
            start(att_send())
            wo_along_done(wo_r)
            start(wo_core())
            att_all[:, my_heads] = att[rows_of(tp), :]

        @pl.when(i == last_att + 2)
        def _():
            arrived(att_send())
            wo_core_done(wo_r)
            total = dot(att_all[:, 0:qw], wo[0])
            for t in range(1, n_tp):
                total = total + dot(att_all[:, t * qw:(t + 1) * qw], wo[t])
            attend_ref[...] = total.astype(BF)

        @pl.when(i >= LAG)
        def _():
            c = i - LAG
            settle(c, c, back_main, back_ext, ret_r)
            e = unfold_ext(back_ext[c], lanes_q)
            slot = iota((tok_m, chunk), 1) + c * chunk
            for k in range(2):
                hot = jnp.where(slot == slot_col[k], 1.0, 0.0).astype(BF)
                acc[k] += dot(hot[:, 0:main_rows], back_main[c])
                for j, piece in enumerate(e):
                    sl = slice(j * 128, (j + 1) * 128)
                    acc[k, :, sl] += dot(hot[:, main_rows:], piece)

        return carry

    lax.fori_loop(0, max(nz + LAG, FIRST_ATT + n_blocks + 2), tick, 0)
    expert_ref[...] = (acc[0] * weight_col[0] + acc[1] * weight_col[1]).astype(BF)

    def drain(i, carry):
        settle(i, i, res_main, res_ext, ret_s)
        for stage in (rs_one, rs_side, rs_two):
            sent(stage(i))
        return carry

    def drain_ag(i, carry):
        settle(i, i, out_main, out_ext, disp_s)
        for stage in (ag_own, ag_fwd):
            sent(stage(i))
        return carry

    def drain_full(i, carry):
        settle(i, full_of(i), full_main, full_ext, disp_s)
        return carry

    lax.fori_loop(0, nz, drain, 0)
    lax.fori_loop(1, n_ag + 1, drain_ag, 0)
    drain_full(0, 0)
    lax.fori_loop(n_ag + 1, nz, drain_full, 0)
    for stage in (halo, wo_own, wo_fwd, att_send):
        sent(stage())
    wo_along_done(wo_s)
    wo_core_done(wo_s)


def fused(dims, *args):
    nz, npl, n_tp, tok_m, tok_a, width, ff, qw, kw = dims
    n_full = nz - ORDERS[nz][1]
    qd = width // n_tp
    half = qd // 2
    chunk = npl * (MAIN + EXTRA)
    eb = EXTRA * qd // 128
    qr = tok_a // n_tp
    vm = pltpu.VMEM
    dma = pltpu.SemaphoreType.DMA
    any_spec = pl.BlockSpec(memory_space=pl.ANY)
    vmem_spec = pl.BlockSpec(memory_space=pltpu.VMEM)
    smem_spec = pl.BlockSpec(memory_space=pltpu.SMEM)
    return pl.pallas_call(
        functools.partial(kernel, dims),
        out_shape=(
            jax.ShapeDtypeStruct((qr, width), BF),
            jax.ShapeDtypeStruct((tok_m, qd), BF),
        ),
        in_specs=[vmem_spec] * 8 + [smem_spec] + [any_spec] * 9,
        out_specs=(vmem_spec, vmem_spec),
        scratch_shapes=[
            vm((tok_m, width), BF), vm((width, ff), BF), vm((width, ff), BF), vm((ff, width), BF),
            vm((tok_a, width), BF), vm((width, qw + 2 * kw), BF), vm((n_tp, qw, width), BF),
            vm((tok_m, width), BF),
            vm((nz, npl * MAIN, qd), BF), vm((nz, npl, eb, 128), BF),
            vm((n_full, npl * MAIN, width), BF), vm((n_full, npl, eb * n_tp, 128), BF),
            vm((nz, chunk, width), BF), vm((nz, npl, eb, 128), BF), vm((n_full, npl, eb * n_tp, 128), BF),
            vm((nz, chunk, width), BF),
            vm((nz, 2, chunk, half), BF), vm((nz, 2, chunk, half), BF), vm((nz, 2, chunk, qd), BF),
            vm((nz, npl * MAIN, qd), BF), vm((nz, npl, eb, 128), BF),
            vm((nz, npl * MAIN, qd), BF), vm((nz, npl, eb, 128), BF),
            vm((2, tok_m, qd), F32),
            vm((tok_a, width), BF), vm((tok_a, qw), BF), vm((tok_a + 2 * WINDOW, 2 * kw), BF),
            vm((tok_a, qw), BF), vm((qr, qw * n_tp), BF),
            dma((9,)), dma((nz, 2)), dma((nz, 2)), dma((nz, 2)), dma((nz, 2)),
            dma((nz, 4)), dma((nz, 4)), dma((nz, 6)), dma((nz, 6)),
            dma((2,)), dma((2,)), dma((6,)), dma((6,)), dma((3,)), dma((3,)),
        ],
        compiler_params=pltpu.CompilerParams(
            collective_id=0, has_side_effects=True, vmem_limit_bytes=60 * 1024 * 1024
        ),
        name="fused_layer",
    )(*args)


def per_device(
    planes,
    x_attend, attend_gain, w_query, w_key, w_value, query_gain, key_gain, sink_logit, w_output,
    x_experts, expert_gain, routes, group_prob, expert_prob, w_gate, w_up, w_down,
):
    n_ep, n_tp = lax.axis_size("ep"), lax.axis_size("tp")
    tok_a, width = x_attend.shape
    dims = (
        planes, n_ep // planes, n_tp, x_experts.shape[0], tok_a, width, w_gate.shape[2],
        w_query.shape[1], w_key.shape[1],
    )
    half_dim = HEAD_DIM // 2
    inverse = np.float32(rope_base) ** (-np.arange(0, half_dim, 2, dtype=np.float32) / np.float32(half_dim))
    inverse = np.tile(inverse.astype(np.float32), 256 // half_dim)[None, :]
    return fused(
        dims, routes.T, expert_prob.T, group_prob[None, :], expert_gain[None, :], attend_gain[None, :],
        query_gain[None, :], key_gain[None, :], inverse,
        sink_logit, x_experts, w_gate, w_up, w_down, x_attend, w_query, w_key, w_value, w_output,
    )


def solution(mesh, planes=8):
    placed = (
        P("ep", None), P(), P(None, "tp"), P(None, "tp"), P(None, "tp"), P(), P(), P("tp"),
        P("tp", None), P("ep", None), P(), P("ep", None), P("ep"), P("ep", None),
        P("ep", None, "tp"), P("ep", None, "tp"), P("ep", "tp", None),
    )
    return jax.shard_map(
        functools.partial(per_device, planes),
        mesh=mesh,
        in_specs=placed,
        out_specs=(P(("ep", "tp"), None), P("ep", "tp")),
        check_vma=False,
    )
```

```python
import functools

import jax
import jax.numpy as jnp
import numpy as np
from jax import lax
from jax.experimental import pallas as pl
from jax.experimental.pallas import tpu as pltpu
from jax.sharding import PartitionSpec as P

HEAD_DIM = 64
WINDOW = 128
GRID_W = 64
MAIN = 16
EXTRA = 2
FIRST_ATT = 3
LAG = 7

epsilon = 1e-06
rope_base = 10000.0

BF = jnp.bfloat16
F32 = jnp.float32
MESH = pl.DeviceIdType.MESH


def dot(a, b):
    return jnp.dot(a, b, preferred_element_type=F32)


def iota(shape, dim):
    return lax.broadcasted_iota(jnp.int32, shape, dim)


ORDERS = {8: ((0, 3, 5, 4, 6, 2, 1, 7), 5), 4: ((0, 2, 1, 3), 2), 2: ((0, 1), 1)}


def kernel(dims, *refs):
    nz, npl, n_tp, tok_m, tok_a, width, ff, qw, kw = dims
    (
        routes_ref, prob_ref, gprob_ref, egain_ref, again_ref, qgain_ref, kgain_ref, inv_ref, sink_ref,
        xm_hbm, wg_hbm, wu_hbm, wd_hbm, xa_hbm, wq_hbm, wk_hbm, wv_hbm, wo_hbm,
        attend_ref, expert_ref,
        xm, wg, wu, wd, xa, wqkv, wo,
        own, out_main, out_ext, full_main, full_ext, grid_in, ext_in, fext_in, hid, wdq, relay,
        res_main, res_ext, back_main, back_ext, acc, normed, qs, kv, att, att_all,
        load_sem, disp_s, disp_r, ret_s, ret_r, ag_s, ag_r, hg_s, hg_r, halo_s, halo_r, wo_s, wo_r, at_s, at_r, wd_s, wd_r,
    ) = refs
    order, n_ag = ORDERS[nz]
    qd = width // n_tp
    half = qd // 2
    main_rows, ext_rows = npl * MAIN, npl * EXTRA
    chunk = main_rows + ext_rows
    eb = EXTRA * qd // 128
    n_ep = nz * npl
    ep = lax.axis_index("ep")
    tp = lax.axis_index("tp")
    z = ep // npl
    p = ep % npl
    nx = npl // 2
    xc, core = p // 2, p % 2
    right, left, opp = (tp + 1) % n_tp, (tp + n_tp - 1) % n_tp, (tp + 2) % n_tp
    after, before = (ep + 1) % n_ep, (ep + n_ep - 1) % n_ep

    barrier = pltpu.get_barrier_semaphore()

    def greet(k, carry):
        pl.semaphore_signal(barrier, inc=1, device_id={"ep": (ep + k) % n_ep}, device_id_type=MESH)
        return carry

    loads = [
        (xm_hbm, xm), (wd_hbm.at[0], wd), (wo_hbm, wo.at[tp]), (xa_hbm, xa), (wq_hbm, wqkv.at[:, 0:qw]), (wk_hbm, wqkv.at[:, qw:qw + kw]),
        (wv_hbm, wqkv.at[:, qw + kw:qw + 2 * kw]),
        (wg_hbm.at[0], wg), (wu_hbm.at[0], wu),
    ]
    loads = [pltpu.make_async_copy(s, d, load_sem.at[i]) for i, (s, d) in enumerate(loads)]
    loads[0].start()
    lax.fori_loop(1, n_ep, greet, 0)
    for side in (left, right, opp):
        pl.semaphore_signal(barrier, inc=1, device_id={"tp": side}, device_id_type=MESH)
    for copy in loads[1:]:
        copy.start()

    ids = [routes_ref[k:k + 1, :] for k in range(2)]
    experts = iota((n_ep, tok_m), 0)
    tri = jnp.where(iota((tok_m, tok_m), 0) < iota((tok_m, tok_m), 1), 1.0, 0.0).astype(BF)
    slot_row = []
    base = None
    for r in ids:
        hot = experts == r
        hot_b = jnp.where(hot, 1.0, 0.0).astype(BF)
        ranks = dot(hot_b, tri)
        if base is None:
            base = jnp.sum(hot_b.astype(F32), axis=1, keepdims=True)
        else:
            ranks = ranks + base
        rank = jnp.sum(jnp.where(hot, ranks, 0.0), axis=0, keepdims=True).astype(jnp.int32)
        dz = lax.rem((r // npl) - z + nz, nz)
        index = jnp.zeros_like(r)
        for i, d in enumerate(order):
            index = jnp.where(dz == d, i, index)
        place = lax.rem(r, npl)
        inside = jnp.where(rank < MAIN, place * MAIN + rank, main_rows + place * EXTRA + rank - MAIN)
        slot_row.append(index * chunk + inside)

    loads[0].wait()
    col0 = pl.multiple_of(tp * qd, 128)

    def norm_m(b, carry):
        rows = pl.ds(pl.multiple_of(b * 32, 32), 32)
        v = xm[rows, :].astype(F32)
        scale = lax.rsqrt(jnp.mean(v * v, axis=-1, keepdims=True) + epsilon)
        own[rows, :] = (v * scale * egain_ref[...]).astype(BF)
        return carry

    lax.fori_loop(0, tok_m // 32, norm_m, 0)
    loads[1].wait()
    loads[2].wait()
    pl.semaphore_wait(barrier, n_ep - 1 + 3)

    def delta(i):
        code = sum(d << (3 * k) for k, d in enumerate(order))
        return lax.rem(lax.shift_right_logical(jnp.int32(code), 3 * i), 8)

    def fold_ext(e, blocks):
        n = npl * EXTRA * blocks
        total = jnp.zeros((n, 128), F32)
        r = iota((n, ext_rows), 0)
        c = iota((n, ext_rows), 1)
        for j in range(blocks):
            pick = jnp.where((r // blocks == c) & (lax.rem(r, blocks) == j), 1.0, 0.0).astype(BF)
            total = total + dot(pick, e[:, j * 128:(j + 1) * 128])
        return total.reshape(npl, EXTRA * blocks, 128).astype(BF)

    def unfold_ext(x, blocks):
        n = npl * EXTRA * blocks
        flat = x.astype(F32).reshape(n, 128).astype(BF)
        r = iota((ext_rows, n), 0)
        c = iota((ext_rows, n), 1)
        out = []
        for j in range(blocks):
            pick = jnp.where(r * blocks + j == c, 1.0, 0.0).astype(BF)
            out.append(dot(pick, flat).astype(BF))
        return out

    def exchange(i, m, main, ext, land_main, land_ext, sems, recv, dest_z):
        def body(k, carry):
            q = lax.rem(p + k, npl)
            dev = {"ep": dest_z * npl + q}
            pltpu.make_async_remote_copy(
                src_ref=main.at[m, pl.ds(pl.multiple_of(q * MAIN, MAIN), MAIN), :],
                dst_ref=land_main, send_sem=sems.at[i, 0], recv_sem=recv.at[i, 0],
                device_id=dev, device_id_type=MESH,
            ).start()
            pltpu.make_async_remote_copy(
                src_ref=ext.at[m, q], dst_ref=land_ext, send_sem=sems.at[i, 1],
                recv_sem=recv.at[i, 1], device_id=dev, device_id_type=MESH,
            ).start()
            return carry

        lax.fori_loop(1 - jnp.minimum(i, 1), npl, body, 0)

    def settle(i, m, main, ext, sems):
        for j, ref in ((0, main), (1, ext)):
            full = ref.at[m]
            few = ref.at[m, 0:(npl - 1) * MAIN, :] if j == 0 else ref.at[m, 0:npl - 1]

            @pl.when(i > 0)
            def _():
                pltpu.make_async_copy(full, full, sems.at[i, j]).wait()

            @pl.when(i == 0)
            def _():
                pltpu.make_async_copy(few, few, sems.at[i, j]).wait()

    my_main = pl.ds(pl.multiple_of(p * MAIN, MAIN), MAIN)
    my_cols = pl.ds(col0, qd)
    lanes_q, lanes_f = qd // 128, width // 128

    def hot_rows(i):
        slot = iota((chunk, tok_m), 0) + i * chunk
        return jnp.where((slot == slot_row[0]) | (slot == slot_row[1]), 1.0, 0.0).astype(BF)

    def full_of(i):
        return jnp.maximum(i - n_ag, 0)

    def dispatch(i, carry):
        rows = dot(hot_rows(i), own[:, my_cols]).astype(BF)
        out_main[i] = rows[0:main_rows]
        out_ext[i] = fold_ext(rows[main_rows:], lanes_q)
        exchange(
            i, i, out_main, out_ext, grid_in.at[i, my_main, my_cols], ext_in.at[i, p],
            disp_s, disp_r, lax.rem(z + delta(i), nz),
        )
        return carry

    def dispatch_full(i, carry):
        d = full_of(i)
        rows = dot(hot_rows(i), own[...]).astype(BF)
        full_main[d] = rows[0:main_rows]
        full_ext[d] = fold_ext(rows[main_rows:], lanes_f)
        exchange(
            i, d, full_main, full_ext, grid_in.at[i, my_main, :], fext_in.at[d, p],
            disp_s, disp_r, lax.rem(z + delta(i), nz),
        )
        return carry

    def start(copies):
        for c in copies:
            c.start()

    def arrived(copies):
        for c in copies:
            c.wait_recv()

    def sent(copies):
        for c in copies:
            c.wait_send()

    def remote(src, dst, sems, recv, dev):
        return pltpu.make_async_remote_copy(
            src_ref=src, dst_ref=dst, send_sem=sems, recv_sem=recv, device_id=dev,
            device_id_type=MESH,
        )

    hw = width // 2
    hrows = qw // 2
    srows = hrows // nx
    my_slice = pl.ds(pl.multiple_of(core * hrows + xc * srows, 16), srows)
    my_half = pl.ds(pl.multiple_of(core * hrows, 16), hrows)

    def wo_own():
        ref = wo.at[tp, my_slice, :]
        return [remote(ref, ref, wo_s.at[k], wo_r.at[k], {"tp": d}) for k, d in ((0, right), (1, left))]

    def wo_fwd():
        a = wo.at[left, my_slice, 0:hw]
        b = wo.at[right, my_slice, hw:width]
        return [
            remote(a, a, wo_s.at[2], wo_r.at[2], {"tp": right}),
            remote(b, b, wo_s.at[3], wo_r.at[3], {"tp": left}),
        ]

    def wo_along():
        out = []
        for k in range(1, nx):
            dev = {"ep": z * npl + lax.rem(xc + k, nx) * 2 + core}
            for shard in (right, left, opp):
                ref = wo.at[shard, my_slice, :]
                out.append(remote(ref, ref, wo_s.at[4], wo_r.at[4], dev))
        return out

    def wo_along_done(sems):
        if nx > 1:
            ref = wo.at[0:3, 0:(nx - 1) * srows, :]
            pltpu.make_async_copy(ref, ref, sems.at[4]).wait()

    def wo_core():
        out = []
        for shard in (right, left, opp):
            ref = wo.at[shard, my_half, :]
            out.append(remote(ref, ref, wo_s.at[5], wo_r.at[5], {"ep": z * npl + xc * 2 + 1 - core}))
        return out

    def wo_core_done(sems):
        ref = wo.at[0:3, 0:hrows, :]
        pltpu.make_async_copy(ref, ref, sems.at[5]).wait()

    def cols(quarter, off, size):
        return pl.ds(pl.multiple_of(quarter * qd + off, 128), size)

    def wd_rows(t):
        return pl.ds(pl.multiple_of(t * ff, 128), ff)

    def wd_own():
        mine = wd_rows(tp)
        return [
            remote(wd.at[:, cols(right, 0, qd)], wdq.at[mine, :], wd_s.at[0], wd_r.at[0], {"tp": right}),
            remote(wd.at[:, cols(left, 0, qd)], wdq.at[mine, :], wd_s.at[1], wd_r.at[1], {"tp": left}),
            remote(wd.at[:, cols(opp, 0, half)], relay.at[0], wd_s.at[2], wd_r.at[2], {"tp": right}),
            remote(wd.at[:, cols(opp, half, half)], relay.at[1], wd_s.at[3], wd_r.at[3], {"tp": left}),
        ]

    def wd_fwd():
        return [
            remote(relay.at[0], wdq.at[wd_rows(left), 0:half], wd_s.at[4], wd_r.at[4], {"tp": right}),
            remote(relay.at[1], wdq.at[wd_rows(right), half:qd], wd_s.at[5], wd_r.at[5], {"tp": left}),
        ]

    start(wd_own())
    start(wo_own())
    lax.fori_loop(1, min(3, n_ag + 1), dispatch, 0)
    dispatch_full(0, 0)
    lax.fori_loop(min(3, n_ag + 1), n_ag + 1, dispatch, 0)
    lax.fori_loop(n_ag + 1, nz, dispatch_full, 0)
    grid_in[0, my_main, :] = full_main[0, my_main, :]
    fext_in[0, p] = full_ext[0, p]
    acc[...] = jnp.zeros_like(acc)

    eye = iota((tok_m, tok_m), 0) == iota((tok_m, tok_m), 1)

    def column(row):
        return jnp.sum(jnp.where(eye, row, 0.0), axis=1, keepdims=True)

    slot_col = [column(r.astype(F32)).astype(jnp.int32) for r in slot_row]
    probs = [prob_ref[k:k + 1, :] for k in range(2)]
    weight_col = [column(gprob_ref[...][None, :] * q / (probs[0] + probs[1])) for q in probs]

    def ag_own(i):
        block = grid_in.at[i, :, my_cols]
        return [
            remote(block, block, ag_s.at[i, s], ag_r.at[i, s], {"tp": d}) for s, d in ((0, right), (1, left))
        ]

    def ag_fwd(i):
        a = grid_in.at[i, :, cols(left, 0, half)]
        b = grid_in.at[i, :, cols(right, half, half)]
        return [
            remote(a, a, ag_s.at[i, 2], ag_r.at[i, 2], {"tp": right}),
            remote(b, b, ag_s.at[i, 3], ag_r.at[i, 3], {"tp": left}),
        ]

    hf = ff // 2

    def units(t, off, size):
        return pl.ds(pl.multiple_of(t * ff + off, 128), size)

    def hg_own(i):
        block = hid.at[i, :, units(tp, 0, ff)]
        return [
            remote(block, block, hg_s.at[i, s], hg_r.at[i, s], {"tp": d}) for s, d in ((0, right), (1, left))
        ]

    def hg_fwd(i):
        a = hid.at[i, :, units(left, 0, hf)]
        b = hid.at[i, :, units(right, hf, hf)]
        return [
            remote(a, a, hg_s.at[i, 2], hg_r.at[i, 2], {"tp": right}),
            remote(b, b, hg_s.at[i, 3], hg_r.at[i, 3], {"tp": left}),
        ]

    quarter_rows = tok_a // n_tp

    def rows_of(t):
        return pl.ds(pl.multiple_of(t * quarter_rows, quarter_rows), quarter_rows)

    my_heads = pl.ds(pl.multiple_of(tp * qw, 128), qw)

    def att_send():
        return [
            remote(att.at[rows_of(d), :], att_all.at[:, my_heads], at_s.at[k], at_r.at[k], {"tp": d})
            for k, d in enumerate((right, left, opp))
        ]

    def halo():
        low, high = kv.at[0:WINDOW, :], kv.at[tok_a + WINDOW:tok_a + 2 * WINDOW, :]
        return [
            remote(kv.at[tok_a:tok_a + WINDOW, :], low, halo_s.at[0], halo_r.at[0], {"ep": after}),
            remote(kv.at[WINDOW:2 * WINDOW, :], high, halo_s.at[1], halo_r.at[1], {"ep": before}),
        ]

    half_dim = HEAD_DIM // 2

    def qkv_all():
        for copy in loads[3:7]:
            copy.wait()
        inv = inv_ref[...]
        q_gain = jnp.concatenate([qgain_ref[...]] * 2, axis=1)
        k_gain = jnp.concatenate([kgain_ref[...]] * 2, axis=1)
        lane = lax.rem(iota((GRID_W, 128), 1), half_dim)
        is_row = lane < half_dim // 2
        col_ang = iota((GRID_W, 128), 0).astype(F32) * inv
        groups = tok_a // GRID_W
        row_ang = (iota((groups, 128), 0) + ep * groups).astype(F32) * inv
        col_cos, col_sin = jnp.cos(col_ang), jnp.sin(col_ang)
        row_cos, row_sin = jnp.cos(row_ang), jnp.sin(row_ang)
        first = lax.rem(iota((1, 128), 1), HEAD_DIM) < half_dim
        sign = jnp.where(first, -1.0, 1.0)
        tables = []
        for g in range(groups):
            c = jnp.where(is_row, row_cos[g:g + 1, :], col_cos)
            s = jnp.where(is_row, row_sin[g:g + 1, :], col_sin) * sign
            tables.append((c, s))
        ones = jnp.where(iota((128, 128), 0) // HEAD_DIM == iota((128, 128), 1) // HEAD_DIM, 1.0, 0.0).astype(BF)

        def rotated(v, gain, c, s):
            sq = v * v
            hi = sq.astype(BF)
            lo = (sq - hi.astype(F32)).astype(BF)
            mean = (dot(hi, ones) + dot(lo, ones)) * (1.0 / HEAD_DIM)
            scaled = v * lax.rsqrt(mean + epsilon) * gain
            other = jnp.where(first, pltpu.roll(scaled, 128 - half_dim, 1), pltpu.roll(scaled, half_dim, 1))
            return (scaled * c + other * s).astype(BF)

        blk = 128
        for b in range(tok_a // blk):
            def norm_a(j, carry):
                rows = pl.ds(pl.multiple_of(b * blk + j * 32, 32), 32)
                v = xa[rows, :].astype(F32)
                scale = lax.rsqrt(jnp.mean(v * v, axis=-1, keepdims=True) + epsilon)
                normed[rows, :] = (v * scale * again_ref[...]).astype(BF)
                return carry

            lax.fori_loop(0, blk // 32, norm_a, 0)
            rows = slice(b * blk, (b + 1) * blk)
            proj = dot(normed[rows, :], wqkv[...])
            per = blk // GRID_W
            c = jnp.concatenate([tables[b * per + j][0] for j in range(per)], axis=0)
            s = jnp.concatenate([tables[b * per + j][1] for j in range(per)], axis=0)
            for j in range(qw // 128):
                sl = slice(j * 128, (j + 1) * 128)
                qs[rows, sl] = rotated(proj[:, sl], q_gain, c, s)
            dst = slice(WINDOW + b * blk, WINDOW + (b + 1) * blk)
            kv[dst, 0:kw] = rotated(proj[:, qw:qw + kw], k_gain, c, s)
            kv[dst, kw:2 * kw] = proj[:, qw + kw:qw + 2 * kw].astype(BF)

    kv_local = kw // HEAD_DIM
    group = qw // kw
    total_len = tok_a * n_ep
    span = 3 * WINDOW

    def attend(b):
        row0 = pl.multiple_of(b * WINDOW, WINDOW)
        q_rows = pl.ds(row0, WINDOW)
        k_rows = pl.ds(row0, span)
        gap = iota((WINDOW, span), 1) - iota((WINDOW, span), 0)
        pos = ep * tok_a - WINDOW + row0 + iota((WINDOW, span), 1)
        valid = (gap >= 0) & (gap <= 2 * WINDOW) & (pos >= 0) & (pos < total_len)
        for h in range(kv_local):
            keys = kv[k_rows, h * HEAD_DIM:(h + 1) * HEAD_DIM]
            vals = kv[k_rows, kw + h * HEAD_DIM:kw + (h + 1) * HEAD_DIM]
            for g in range(group):
                head = h * group + g
                lanes = slice(head * HEAD_DIM, (head + 1) * HEAD_DIM)
                q = qs[q_rows, lanes]
                s = lax.dot_general(q, keys, (((1,), (1,)), ((), ())), preferred_element_type=F32)
                s = jnp.where(valid, s * HEAD_DIM ** (-0.5), -1e30)
                sink = sink_ref[head]
                peak = jnp.maximum(jnp.max(s, axis=-1, keepdims=True), sink)
                w = jnp.exp(s - peak)
                denom = jnp.sum(w, axis=-1, keepdims=True) + jnp.exp(sink - peak)
                weights = (w * (1.0 / denom)).astype(BF)
                att[q_rows, lanes] = dot(weights, vals).astype(BF)

    n_blocks = tok_a // WINDOW

    qkv_all()
    start(halo())

    def staged(i, lag):
        return (i == lag - 1) | ((i > lag) & (i < nz + lag)), jnp.maximum(i - lag, 0)

    def tick(i, carry):
        @pl.when(i < n_ag)
        def _():
            c = i + 1
            settle(c, c, out_main, ext_in, disp_r)
            for j, piece in enumerate(unfold_ext(ext_in[c], lanes_q)):
                grid_in[c, main_rows:chunk, cols(tp, j * 128, 128)] = piece
            start(ag_own(c))

        @pl.when(i == 0)
        def _():
            arrived(wd_own())
            start(wd_fwd())
            wdq[wd_rows(tp), :] = wd[:, my_cols]
            arrived(wo_own())
            start(wo_fwd())

        @pl.when((i >= 1) & (i < n_ag + 1))
        def _():
            arrived(ag_own(i))
            start(ag_fwd(i))

        @pl.when(i == 1)
        def _():
            arrived(wo_fwd())
            start(wo_along())

        ffn_on, ffn_c = staged(i, 1)

        @pl.when(ffn_on)
        def _():
            c = ffn_c

            @pl.when(c == 0)
            def _():
                for copy in loads[7:9]:
                    copy.wait()

            direct = (c == 0) | (c > n_ag)

            @pl.when(direct)
            def _():
                d = full_of(c)
                settle(c, d, full_main, fext_in, disp_r)
                for j, piece in enumerate(unfold_ext(fext_in[d], lanes_f)):
                    grid_in[c, main_rows:chunk, j * 128:(j + 1) * 128] = piece

            @pl.when(jnp.logical_not(direct))
            def _():
                arrived(ag_fwd(c))

            x = grid_in[c]
            g = dot(x, wg[...])
            u = dot(x, wu[...])
            hid[c, :, units(tp, 0, ff)] = (g / (1.0 + jnp.exp(-g)) * u).astype(BF)
            start(hg_own(c))

        mid_on, mid_c = staged(i, 2)

        @pl.when(mid_on)
        def _():
            c = mid_c
            arrived(hg_own(c))
            start(hg_fwd(c))

        fin_on, fin_c = staged(i, 3)

        @pl.when(fin_on)
        def _():
            c = fin_c
            @pl.when(c == 0)
            def _():
                arrived(wd_fwd())

            arrived(hg_fwd(c))
            total = dot(hid[c], wdq[...]).astype(BF)
            res_main[c] = total[0:main_rows]
            res_ext[c] = fold_ext(total[main_rows:], lanes_q)
            exchange(
                c, c, res_main, res_ext, back_main.at[c, my_main, :], back_ext.at[c, p],
                ret_s, ret_r, lax.rem(z - delta(c) + nz, nz),
            )

            @pl.when(c == 0)
            def _():
                back_main[0, my_main, :] = res_main[0, my_main, :]
                back_ext[0, p] = res_ext[0, p]

        @pl.when(i == FIRST_ATT)
        def _():
            arrived(halo())

        @pl.when((i >= FIRST_ATT) & (i < FIRST_ATT + n_blocks))
        def _():
            attend(i - FIRST_ATT)

        last_att = FIRST_ATT + n_blocks - 1

        @pl.when(i == last_att)
        def _():
            start(att_send())
            wo_along_done(wo_r)
            start(wo_core())
            att_all[:, my_heads] = att[rows_of(tp), :]

        @pl.when(i == last_att + 2)
        def _():
            arrived(att_send())
            wo_core_done(wo_r)
            total = dot(att_all[:, 0:qw], wo[0])
            for t in range(1, n_tp):
                total = total + dot(att_all[:, t * qw:(t + 1) * qw], wo[t])
            attend_ref[...] = total.astype(BF)

        @pl.when(i >= LAG)
        def _():
            c = i - LAG
            settle(c, c, back_main, back_ext, ret_r)
            e = unfold_ext(back_ext[c], lanes_q)
            slot = iota((tok_m, chunk), 1) + c * chunk
            for k in range(2):
                hot = jnp.where(slot == slot_col[k], 1.0, 0.0).astype(BF)
                acc[k] += dot(hot[:, 0:main_rows], back_main[c])
                for j, piece in enumerate(e):
                    sl = slice(j * 128, (j + 1) * 128)
                    acc[k, :, sl] += dot(hot[:, main_rows:], piece)

        return carry

    lax.fori_loop(0, max(nz + LAG, FIRST_ATT + n_blocks + 2), tick, 0)
    expert_ref[...] = (acc[0] * weight_col[0] + acc[1] * weight_col[1]).astype(BF)

    def drain(i, carry):
        settle(i, i, res_main, res_ext, ret_s)
        for stage in (hg_own, hg_fwd):
            sent(stage(i))
        return carry

    def drain_ag(i, carry):
        settle(i, i, out_main, out_ext, disp_s)
        for stage in (ag_own, ag_fwd):
            sent(stage(i))
        return carry

    def drain_full(i, carry):
        settle(i, full_of(i), full_main, full_ext, disp_s)
        return carry

    lax.fori_loop(0, nz, drain, 0)
    lax.fori_loop(1, n_ag + 1, drain_ag, 0)
    drain_full(0, 0)
    lax.fori_loop(n_ag + 1, nz, drain_full, 0)
    for stage in (halo, wo_own, wo_fwd, wd_own, wd_fwd, att_send):
        sent(stage())
    wo_along_done(wo_s)
    wo_core_done(wo_s)


def fused(dims, *args):
    nz, npl, n_tp, tok_m, tok_a, width, ff, qw, kw = dims
    n_full = nz - ORDERS[nz][1]
    qd = width // n_tp
    half = qd // 2
    chunk = npl * (MAIN + EXTRA)
    eb = EXTRA * qd // 128
    qr = tok_a // n_tp
    vm = pltpu.VMEM
    dma = pltpu.SemaphoreType.DMA
    any_spec = pl.BlockSpec(memory_space=pl.ANY)
    vmem_spec = pl.BlockSpec(memory_space=pltpu.VMEM)
    smem_spec = pl.BlockSpec(memory_space=pltpu.SMEM)
    return pl.pallas_call(
        functools.partial(kernel, dims),
        out_shape=(pltpu.VMEM((qr, width), BF), pltpu.VMEM((tok_m, qd), BF)),
        in_specs=[vmem_spec] * 8 + [smem_spec] + [any_spec] * 9,
        out_specs=(vmem_spec, vmem_spec),
        scratch_shapes=[
            vm((tok_m, width), BF), vm((width, ff), BF), vm((width, ff), BF), vm((ff, width), BF),
            vm((tok_a, width), BF), vm((width, qw + 2 * kw), BF), vm((n_tp, qw, width), BF),
            vm((tok_m, width), BF),
            vm((nz, npl * MAIN, qd), BF), vm((nz, npl, eb, 128), BF),
            vm((n_full, npl * MAIN, width), BF), vm((n_full, npl, eb * n_tp, 128), BF),
            vm((nz, chunk, width), BF), vm((nz, npl, eb, 128), BF), vm((n_full, npl, eb * n_tp, 128), BF),
            vm((nz, chunk, ff * n_tp), BF), vm((ff * n_tp, qd), BF), vm((2, ff, half), BF),
            vm((nz, npl * MAIN, qd), BF), vm((nz, npl, eb, 128), BF),
            vm((nz, npl * MAIN, qd), BF), vm((nz, npl, eb, 128), BF),
            vm((2, tok_m, qd), F32),
            vm((tok_a, width), BF), vm((tok_a, qw), BF), vm((tok_a + 2 * WINDOW, 2 * kw), BF),
            vm((tok_a, qw), BF), vm((qr, qw * n_tp), BF),
            dma((9,)), dma((nz, 2)), dma((nz, 2)), dma((nz, 2)), dma((nz, 2)),
            dma((nz, 4)), dma((nz, 4)), dma((nz, 4)), dma((nz, 4)),
            dma((2,)), dma((2,)), dma((6,)), dma((6,)), dma((3,)), dma((3,)), dma((6,)), dma((6,)),
        ],
        compiler_params=pltpu.CompilerParams(
            collective_id=0, has_side_effects=True, vmem_limit_bytes=60 * 1024 * 1024
        ),
        name="fused_layer",
    )(*args)


def per_device(
    planes,
    x_attend, attend_gain, w_query, w_key, w_value, query_gain, key_gain, sink_logit, w_output,
    x_experts, expert_gain, routes, group_prob, expert_prob, w_gate, w_up, w_down,
):
    n_ep, n_tp = lax.axis_size("ep"), lax.axis_size("tp")
    tok_a, width = x_attend.shape
    dims = (
        planes, n_ep // planes, n_tp, x_experts.shape[0], tok_a, width, w_gate.shape[2],
        w_query.shape[1], w_key.shape[1],
    )
    half_dim = HEAD_DIM // 2
    inverse = np.float32(rope_base) ** (-np.arange(0, half_dim, 2, dtype=np.float32) / np.float32(half_dim))
    inverse = np.tile(inverse.astype(np.float32), 256 // half_dim)[None, :]
    return fused(
        dims, routes.T, expert_prob.T, group_prob, expert_gain[None, :], attend_gain[None, :],
        query_gain[None, :], key_gain[None, :], inverse,
        sink_logit, x_experts, w_gate, w_up, w_down, x_attend, w_query, w_key, w_value, w_output,
    )


def solution(mesh, planes=8):
    placed = (
        P("ep", None), P(), P(None, "tp"), P(None, "tp"), P(None, "tp"), P(), P(), P("tp"),
        P("tp", None), P("ep", None), P(), P("ep", None), P("ep"), P("ep", None),
        P("ep", None, "tp"), P("ep", None, "tp"), P("ep", "tp", None),
    )
    return jax.shard_map(
        functools.partial(per_device, planes),
        mesh=mesh,
        in_specs=placed,
        out_specs=(P(("ep", "tp"), None), P("ep", "tp")),
        check_vma=False,
    )
```
